32 devices in a mesh: sp: 8 (over z, y), tp: 4 (over x, core).
Axes of the slice: x: 2, y: 2, z: 4, core: 2. Of those that a mesh axis runs over, the one named last changes fastest.
Arguments:
- queries: bfloat16 [4096, 1024], P('sp', 'tp'), may hold values from -6 to 6
- keys: bfloat16 [4096, 1024], P('sp', 'tp'), may hold values from -6 to 6
- values: bfloat16 [4096, 1024], P('sp', 'tp'), may hold values from -6 to 6
- cum_gate: float32 [4096, 16], P('sp', 'tp'), as said below
- documents: int32 [4096], P('sp'), may hold values from 0 to 3, never falling along the last dimension, each value on 1 to 2048 neighbouring positions
- head_gain: float32 [1024], P('tp'), may hold values from 0.1 to 1.9
- out_weight: bfloat16 [1024, 2048], replicated, may hold values from -0.1875 to 0.1875
- resid: bfloat16 [4096, 2048], P(('sp', 'tp')), may hold values from -6 to 6
- norm_gain: float32 [2048], replicated, may hold values from 0.1 to 1.9
- routes: int32 [4096, 2], P(('sp', 'tp')), may hold values from 0 to 7, all different within a row; in each aligned block of 128 rows (0 to 127, 128 to 255, ...) at most 64 rows name the same one
- route_weights: float32 [4096, 2], P(('sp', 'tp')), may hold values from 0.25 to 1
- w_gate: bfloat16 [8, 2048, 3584], P('sp', None, 'tp'), may hold values from -0.125 to 0.125
- w_up: bfloat16 [8, 2048, 3584], P('sp', None, 'tp'), may hold values from -0.125 to 0.125
- w_down: bfloat16 [8, 3584, 2048], P('sp', 'tp'), may hold values from -0.09375 to 0.09375
Outputs:
- mixed: bfloat16 [4096, 2048], P(('sp', 'tp'))
The draws below stay inside these ranges and needn't reach their ends.
Inputs may be any that keep to these rules, and one draw needn't show every extreme that they name: `cum_gate`: along the positions each head's values never rise. `documents`: document numbers never fall along the positions. `routes`: the 2 experts of a row differ. In each aligned block of 128 rows no expert is named more than 64 times; in some blocks an expert is named exactly 64 times.
All inputs are finite; a program needn't handle non-finite values.
Results may differ from the reference program's by a relative error of at most 0.015.
Values may be sent and summed in bfloat16 or wider, within the bound.
No kernel may reach another device: no remote copies, remote signals or barrier semaphores. Data moves between devices by JAX's collectives and lax.ppermute only.
A program may use at most 128 MiB of HBM per device.

```python
import math
import jax
import jax.numpy as jnp
import numpy as np
from jax import lax

D = 2048
HEADS = 16
HEAD_DIM = 64
FFE = 3584
TOP = 2
TOK_DEV = 512
SEQUENCE_LENGTH = 4096
ROWS_DEV = 128
HD = 1024
EXPERTS = 8
CAP = 64
SLICE = 896
N_SP = 8
N_TP = 4


def draw_queries(key, part):
    drawn = jax.random.normal(jax.random.fold_in(key, 1), (SEQUENCE_LENGTH, HEADS * HEAD_DIM), jnp.float32)
    return jnp.clip(drawn, -6.0, 6.0).astype(jnp.bfloat16)


def draw_keys(key, part):
    drawn = jax.random.normal(jax.random.fold_in(key, 2), (SEQUENCE_LENGTH, HEADS * HEAD_DIM), jnp.float32)
    return jnp.clip(drawn, -6.0, 6.0).astype(jnp.bfloat16)


def draw_cum_gate(key, part):
    head_order = jax.random.permutation(jax.random.fold_in(key, 21), HEADS)
    fast_heads = head_order < HEADS // 2
    quick_decay_rate = jnp.exp(jax.random.uniform(jax.random.fold_in(key, 22), (HEADS,), jnp.float32, math.log(0.03), math.log(0.08)))
    slow_rate = jax.random.uniform(jax.random.fold_in(key, 23), (HEADS,), jnp.float32, 0.3, 0.8) / SEQUENCE_LENGTH
    head_rates = jnp.where(fast_heads, quick_decay_rate, slow_rate)
    blocks = SEQUENCE_LENGTH // TOK_DEV
    factor = jnp.exp(jax.random.uniform(jax.random.fold_in(key, 24), (blocks, HEADS), jnp.float32, -0.7, 0.7))
    factor = jnp.repeat(factor, TOK_DEV, axis=0)
    jitter = jax.random.uniform(jax.random.fold_in(key, 25), (SEQUENCE_LENGTH, HEADS), jnp.float32, 0.5, 1.5)
    logged_step_list = -head_rates[None, :] * factor * jitter
    spike_position = jax.random.randint(jax.random.fold_in(key, 26), (3,), 0, SEQUENCE_LENGTH)
    loss_values = jax.random.uniform(jax.random.fold_in(key, 27), (3, HEADS), jnp.float32, 0.2, 0.5)
    logged_step_list = logged_step_list.at[spike_position].add(jnp.log(1.0 - loss_values))
    return jnp.cumsum(logged_step_list, axis=0)


def block_scale(stream_key, shape, shards, smallest, high):
    factor_of = 1.0
    for axis_at, shards_of in shards:
        heights = jax.random.uniform(jax.random.fold_in(jax.random.fold_in(stream_key, 6), axis_at), (shards_of,), jnp.float32, smallest / len(shards), high / len(shards))
        factor_of = factor_of * jnp.repeat(jnp.exp(heights), shape[axis_at] // shards_of).reshape((-1,) + (1,) * (len(shape) - 1 - axis_at))
    return factor_of


def length_profile(count, total, reach, slope):
    loads = [(1 << 20) // math.isqrt(rank ** slope) + 1 for rank in range(2, count + 1)]
    spare, given = total - reach - (count - 1), [1] * (count - 1)
    while spare > 0:
        candidates = [i for i in range(count - 1) if given[i] < reach]
        pool, left = sum([loads[i] for i in candidates]), spare
        for i in candidates:
            addition = min(reach - given[i], max(1, left * loads[i] // pool), spare)
            given[i] = given[i] + addition
            spare = spare - addition
    return np.array([reach] + given)


def ragged_sizes(own_key, count, total, bound, lean):
    if count == 2:
        one = jax.random.randint(own_key, (), max(1, total - bound), min(bound, total - 1) + 1)
        return jnp.stack([one, total - one])
    sizes = jnp.asarray(length_profile(count, total, bound, lean), jnp.int32)
    twos = (count - 1) // 2
    source_of, taker = sizes[1:1 + 2 * twos:2], sizes[2:2 + 2 * twos:2]
    margin = jnp.minimum(source_of - 1, bound - taker)
    shifted = jax.random.randint(jax.random.fold_in(own_key, 1), (twos,), 0, 1 << 20) % (margin + 1)
    sizes = sizes.at[1:1 + 2 * twos:2].set(source_of - shifted).at[2:2 + 2 * twos:2].set(taker + shifted)
    return sizes[jax.random.permutation(jax.random.fold_in(own_key, 2), count)]


def shared_out(own_key, own, number, rows, count, top, most, lean):
    sequence = jax.random.permutation(own_key, count)
    heavy_load, usual = shares(count, rows * top, most, lean, True), shares(count, rows * top, most, lean, False)
    places = jnp.arange(count)

    def named(tallies, offset_by):
        used = int((tallies > 0).sum())
        fixed = max(1, used // 4)
        passed = fixed + (places - fixed + offset_by * (used - fixed)) % max(1, count - fixed)
        return jnp.zeros((count,), jnp.int32).at[sequence[jnp.where(places < fixed, places, passed)]].set(jnp.asarray(tallies, jnp.int32))

    tallies = jnp.where(number % 4 == 0, named(heavy_load, number // 4), named(usual, number - number // 4 - 1))
    mixed = jax.random.permutation(jax.random.fold_in(own, 3), count)
    source_of, sink = mixed[0:count // 2 * 2:2], mixed[1:count // 2 * 2:2]
    room = jnp.minimum(tallies[source_of] - 1, most - tallies[sink]) // 2
    room = jnp.where((source_of == sequence[0]) | (sink == sequence[0]) | (tallies[sink] == 0), 0, jnp.maximum(room, 0))
    passed = jax.random.randint(jax.random.fold_in(own, 4), (count // 2,), 0, 1 << 20) % (room + 1)
    tallies = tallies.at[source_of].add(-passed).at[sink].add(passed)
    labels = jnp.searchsorted(jnp.cumsum(tallies), jnp.arange(rows * top), side="right").astype(jnp.int32)
    table = labels.reshape(top, rows).T
    table = table[jax.random.permutation(jax.random.fold_in(own, 1), rows)]
    offset_by = jax.random.randint(jax.random.fold_in(own, 2), (rows, 1), 0, top)
    return jnp.take_along_axis(table, (jnp.arange(top)[None, :] + offset_by) % top, axis=1)


def shares(amount, total, limit, slope, full):
    portions = [(1 << 20) // math.isqrt(grade ** slope) + 1 for grade in range(1, amount + 1)]
    largest = limit if full else min(limit, max(-(-total // amount), total * portions[0] // sum(portions)))
    least = 1 if total - largest >= amount - 1 else 0
    counts, spare = [largest] + [least] * (amount - 1), total - largest - least * (amount - 1)
    while spare > 0:
        free = [i for i in range(1, amount) if counts[i] < largest] or [i for i in range(1, amount) if counts[i] < limit]
        whole, remaining = sum([portions[i] for i in free]), spare
        for i in free:
            extra = min(limit - counts[i], max(1, remaining * portions[i] // whole), spare)
            counts[i] = counts[i] + extra
            spare = spare - extra
    return np.array(counts)


def noise(stream_key, dims, spread, bound, split=(), held_as=jnp.bfloat16):
    entries = jax.random.normal(stream_key, dims, jnp.float32) * spread
    if len(split) > 0:
        entries = block_scale(stream_key, dims, split, -0.22, 0.18) * entries
    return jnp.clip(entries, min=-bound, max=bound).astype(held_as)


def setup_inputs(seed: int = 0) -> dict:
    seeds = jax.random.split(jax.random.key(seed), 15)
    queries = draw_queries(jax.random.fold_in(seeds[14], 71), 0)
    keys = draw_keys(jax.random.fold_in(seeds[14], 71), 0)
    values = noise(seeds[2], (SEQUENCE_LENGTH, HD), 1.0, 6.0, ((0, 8), (1, 4)))
    cum_gate = draw_cum_gate(jax.random.fold_in(seeds[14], 71), 0)
    documents = jnp.searchsorted(jnp.cumsum(ragged_sizes(seeds[4], 4, SEQUENCE_LENGTH, SEQUENCE_LENGTH // 2, 2)), jnp.arange(SEQUENCE_LENGTH), side="right").astype(jnp.int32)
    head_gain = jnp.clip(1.0 + 0.18 * jax.random.normal(seeds[5], (HD,), jnp.float32), 0.1, 1.9)
    out_weight = noise(seeds[6], (HD, D), HD ** -0.5, 0.1875)
    resid = noise(seeds[7], (SEQUENCE_LENGTH, D), 1.0, 6.0, ((0, 32),))
    norm_gain = jnp.clip(1.0 + 0.18 * jax.random.normal(seeds[8], (D,), jnp.float32), 0.1, 1.9)
    routes_keys = jax.random.split(jax.random.fold_in(seeds[9], 1), SEQUENCE_LENGTH // ROWS_DEV)
    routes_turns = jax.random.permutation(jax.random.fold_in(seeds[9], 3), SEQUENCE_LENGTH // ROWS_DEV)
    routes = jax.vmap(lambda own, number: shared_out(jax.random.fold_in(seeds[9], 2), own, number, ROWS_DEV, EXPERTS, TOP, CAP, 2))(routes_keys, routes_turns).reshape((SEQUENCE_LENGTH, TOP))
    route_weights = jnp.clip(jnp.exp(math.log(1.0) - 1.3862944 * jax.random.uniform(seeds[10], (SEQUENCE_LENGTH, TOP), jnp.float32) ** block_scale(seeds[10], (SEQUENCE_LENGTH, TOP), ((0, 32),), -0.2, 0.2)), 0.25, 1.0)
    w_gate = noise(seeds[11], (EXPERTS, D, FFE), D ** -0.5, 0.125, ((0, 8), (2, 4)))
    w_up = noise(seeds[12], (EXPERTS, D, FFE), D ** -0.5, 0.125, ((0, 8), (2, 4)))
    w_down = noise(seeds[13], (EXPERTS, FFE, D), FFE ** -0.5, 0.09375, ((0, 8), (1, 4)))
    return dict(queries=queries, keys=keys, values=values, cum_gate=cum_gate, documents=documents, head_gain=head_gain, out_weight=out_weight, resid=resid, norm_gain=norm_gain, routes=routes, route_weights=route_weights, w_gate=w_gate, w_up=w_up, w_down=w_down)


EPS = 1e-06

def attention(queries, keys, values, cum_gate, documents):
    block_len = math.gcd(SEQUENCE_LENGTH, 256)
    block_count = SEQUENCE_LENGTH // block_len
    key_heads = keys.reshape(SEQUENCE_LENGTH, HEADS, HEAD_DIM).astype(jnp.float32)
    value_heads = values.reshape(SEQUENCE_LENGTH, HEADS, HEAD_DIM).astype(jnp.float32)
    positions = jnp.arange(SEQUENCE_LENGTH, dtype=jnp.int32)
    score_scale = HEAD_DIM ** (-0.5)

    def one_block(block_index):
        first_pos = block_index * block_len
        query_row_block = lax.dynamic_slice_in_dim(queries, first_pos, block_len, 0)
        query_row_block = query_row_block.reshape(block_len, HEADS, HEAD_DIM).astype(jnp.float32)
        gate_here = lax.dynamic_slice_in_dim(cum_gate, first_pos, block_len, 0)
        doc_here = lax.dynamic_slice_in_dim(documents, first_pos, block_len, 0)
        query_pos = first_pos + jnp.arange(block_len, dtype=jnp.int32)
        scores = jnp.einsum('qhd,khd->qhk', query_row_block, key_heads) * score_scale
        scores = scores + gate_here[:, :, None] - cum_gate.T[None, :, :]
        allowed = (positions[None, :] <= query_pos[:, None]) & (documents[None, :] == doc_here[:, None])
        scores = jnp.where(allowed[:, None, :], scores, -jnp.inf)
        row_max = lax.optimization_barrier(jnp.max(scores, axis=-1, keepdims=True))
        exp_scores = jnp.exp(scores - row_max)
        row_sum = lax.optimization_barrier(jnp.sum(exp_scores, axis=-1))
        weights = lax.optimization_barrier(exp_scores.astype(jnp.bfloat16)).astype(jnp.float32)
        return jnp.einsum('qhk,khd->qhd', weights, value_heads) / row_sum[:, :, None]
    attended = lax.map(one_block, jnp.arange(block_count, dtype=jnp.int32))
    return attended.reshape(SEQUENCE_LENGTH, HEADS, HEAD_DIM)

def experts_out(expert_input, routes, w_gate, w_up, w_down):
    capacity = N_SP * N_TP * CAP
    flat_routes = routes.reshape(-1)
    route_total = flat_routes.shape[0]
    owners = jnp.arange(route_total, dtype=jnp.int32) // TOP

    def one_expert(expert_index):
        matches = (flat_routes == expert_index).astype(jnp.int32)
        ranks = jnp.cumsum(matches) - 1
        slots = jnp.where(matches == 1, ranks, capacity)
        slot_owner = jnp.zeros((capacity + 1,), jnp.int32).at[slots].set(owners)[:capacity]
        picked = expert_input[slot_owner]
        gate_out = jnp.dot(picked, w_gate[expert_index], preferred_element_type=jnp.float32)
        up_out = jnp.dot(picked, w_up[expert_index], preferred_element_type=jnp.float32)
        hidden = (jax.nn.silu(gate_out) * up_out).astype(jnp.bfloat16)
        pieces = hidden.reshape(capacity, N_TP, SLICE).astype(jnp.float32)
        down_blocks = w_down[expert_index].reshape(N_TP, SLICE, D).astype(jnp.float32)
        partial_value = jnp.einsum('rjf,jfd->jrd', pieces, down_blocks)
        partial_value = lax.optimization_barrier(partial_value.astype(jnp.bfloat16)).astype(jnp.float32)
        return lax.optimization_barrier(jnp.sum(partial_value, axis=0)).astype(jnp.bfloat16)
    results = lax.map(one_expert, jnp.arange(EXPERTS, dtype=jnp.int32))
    onehot = (flat_routes[:, None] == jnp.arange(EXPERTS, dtype=jnp.int32)[None, :]).astype(jnp.int32)
    ranks = lax.optimization_barrier(jnp.sum(jnp.cumsum(onehot, axis=0) * onehot, axis=1)) - 1
    return results[flat_routes, ranks].reshape(SEQUENCE_LENGTH, TOP, D)

def reference(queries, keys, values, cum_gate, documents, head_gain, out_weight, resid, norm_gain, routes, route_weights, w_gate, w_up, w_down):
    attended = attention(queries, keys, values, cum_gate, documents)
    mean_square = lax.optimization_barrier(jnp.mean(attended * attended, axis=-1, keepdims=True))
    head_normed = (attended * lax.rsqrt(mean_square + EPS)).reshape(SEQUENCE_LENGTH, HEADS * HEAD_DIM) * head_gain
    head_normed = head_normed.astype(jnp.bfloat16)
    projected = jnp.dot(head_normed, out_weight, preferred_element_type=jnp.float32)
    stream = lax.optimization_barrier((resid.astype(jnp.float32) + projected).astype(jnp.bfloat16))
    widened = stream.astype(jnp.float32)
    mean_wide = lax.optimization_barrier(jnp.mean(widened * widened, axis=-1, keepdims=True))
    expert_input = (widened * lax.rsqrt(mean_wide + EPS) * norm_gain).astype(jnp.bfloat16)
    gathered = experts_out(expert_input, routes, w_gate, w_up, w_down)
    mixed = widened + lax.optimization_barrier(jnp.sum(route_weights[:, :, None] * gathered.astype(jnp.float32), axis=1))
    return mixed.astype(jnp.bfloat16)
```

```python
import math

import jax
import jax.numpy as jnp
from jax import lax
from jax.experimental import pallas as pl
from jax.experimental.pallas import tpu as pltpu
from jax.sharding import PartitionSpec as P

EPS = 1e-06
LOG2E = 1.4426950408889634
NEG = -1e30


def bf16_parts(x):
    hi = lax.reduce_precision(x, 8, 7)
    rest = x - hi
    mid = lax.reduce_precision(rest, 8, 7)
    low = rest - mid
    return [part.astype(jnp.bfloat16) for part in (hi, mid, low)]


def attention_kernel(tokens, heads, head_size, tile, sources, *refs):
    valid_ref, docs_ref, q_ref, meta_ref, gain_ref = refs[:5]
    kv_refs = refs[5 : 5 + 2 * sources]
    out_ref = refs[5 + 2 * sources]
    m_ref, l_ref, acc_ref = refs[6 + 2 * sources :]
    width = heads * head_size
    halves = tokens // width
    rows = tokens // head_size
    score_scale = head_size ** (-0.5) * LOG2E
    lane = lax.broadcasted_iota(jnp.int32, (1, width), 1)
    in_head = [(lane >= h * head_size) & (lane < (h + 1) * head_size) for h in range(heads)]

    def spread(parts):
        full = jnp.broadcast_to(parts[0], (tile, width))
        for h in range(1, heads):
            full = jnp.where(in_head[h], parts[h], full)
        return full

    def q_tile(step, carry):
        row0 = pl.multiple_of(step * tile, tile)
        q = q_ref[pl.ds(row0, tile), :]
        meta = meta_ref[pl.ds(row0, tile), :]
        q_doc = meta[:, heads : heads + 1]
        first_doc = docs_ref[row0].astype(jnp.float32)

        def visit(source):
            k_ref, v_ref = kv_refs[2 * source], kv_refs[2 * source + 1]
            k = k_ref[:tokens, :]
            v = v_ref[...]
            extra = k_ref[tokens:, :].astype(jnp.float32)
            gates = (extra[:rows] + extra[rows : 2 * rows] + extra[2 * rows : 3 * rows]) * LOG2E
            doc_rows = extra[3 * rows : 3 * rows + halves]
            k_doc = jnp.concatenate([doc_rows[j : j + 1] for j in range(halves)], axis=1)
            allowed = k_doc == q_doc
            if source == 0:
                q_pos = row0 + lax.broadcasted_iota(jnp.int32, (tile, tokens), 0)
                k_pos = lax.broadcasted_iota(jnp.int32, (tile, tokens), 1)
                allowed = allowed & (k_pos <= q_pos)
            total = jnp.zeros((tile, width), jnp.float32)
            rescales = []
            for h in range(heads):
                q_h = jnp.where(in_head[h], q, jnp.zeros((), q.dtype))
                s = lax.dot_general(
                    q_h, k, (((1,), (1,)), ((), ())), preferred_element_type=jnp.float32
                )
                gate_row = jnp.concatenate(
                    [gates[h * halves + j : h * halves + j + 1] for j in range(halves)], axis=1
                )
                s = s * score_scale + (meta[:, h : h + 1] * LOG2E - gate_row)
                s = jnp.where(allowed, s, NEG)
                block_max = jnp.max(s, axis=1, keepdims=True)
                if source == 0:
                    new_max = block_max
                else:
                    old_max = m_ref[h]
                    new_max = jnp.maximum(old_max, block_max)
                    rescale = jnp.exp2(old_max - new_max)
                    rescales.append(rescale)
                p = jnp.exp2(s - new_max)
                block_sum = jnp.sum(p, axis=1, keepdims=True)
                m_ref[h] = new_max
                l_ref[h] = block_sum if source == 0 else l_ref[h] * rescale + block_sum
                v_h = jnp.where(in_head[h], v, jnp.zeros((), v.dtype))
                total = total + jnp.dot(
                    p.astype(jnp.bfloat16), v_h, preferred_element_type=jnp.float32
                )
            if source == 0:
                acc_ref[...] = total
            else:
                acc_ref[...] = acc_ref[...] * spread(rescales) + total

        visit(0)
        for source in range(1, sources):
            last_doc = jnp.max(
                kv_refs[2 * source][tokens + 3 * rows : tokens + 3 * rows + halves, :].astype(
                    jnp.float32
                )
            )

            @pl.when((valid_ref[source] > 0) & (last_doc >= first_doc))
            def _():
                visit(source)

        attended = acc_ref[...] / spread([l_ref[h] for h in range(heads)])
        squares = attended * attended
        means = [
            jnp.sum(jnp.where(in_head[h], squares, 0.0), axis=1, keepdims=True) / head_size
            for h in range(heads)
        ]
        scale = spread([lax.rsqrt(mean + EPS) for mean in means])
        out_ref[pl.ds(row0, tile), :] = (attended * scale * gain_ref[...]).astype(jnp.bfloat16)
        return carry

    lax.fori_loop(0, tokens // tile, q_tile, 0)


def attend(queries, keys, values, cum_gate, documents, head_gain):
    tokens, width = queries.shape
    heads = cum_gate.shape[1]
    head_size = width // heads
    n_sp = lax.axis_size("sp")
    place = lax.axis_index("sp")
    tile = math.gcd(tokens, 128)

    gate_rows = [part.T.reshape(-1, width) for part in bf16_parts(cum_gate)]
    doc_rows = documents.astype(jnp.bfloat16).reshape(-1, width)
    used = sum(part.shape[0] for part in gate_rows) + doc_rows.shape[0]
    filler = jnp.zeros((-used % 16, width), jnp.bfloat16)
    keys_more = jnp.concatenate([keys, *gate_rows, doc_rows, filler], axis=0)
    meta = jnp.concatenate(
        [
            cum_gate,
            documents.astype(jnp.float32)[:, None],
            jnp.zeros((tokens, 8 - (heads + 1) % 8), jnp.float32),
        ],
        axis=1,
    )

    reach = n_sp // 4
    ahead = [(i, i + 2) for i in range(n_sp - 2)]
    even_up = [(i, i + 1) for i in range(0, n_sp, 2)]
    odd_down = [(i + 1, i) for i in range(0, n_sp, 2)]

    def chain(first):
        own, other = [first], []
        for step in range(reach + 1):
            pairs = even_up if step == 0 else odd_down if step == reach else even_up + odd_down
            if step > 0:
                own.append(lax.ppermute(own[-1], "sp", ahead))
            other.append(lax.ppermute(own[-1], "sp", pairs))
        return own, other

    key_own, key_other = chain(keys_more)
    value_own, value_other = chain(values)
    group, member = place // 2, place % 2
    blocks, valid = [], []
    for step in range(reach + 1):
        exists = group - step >= 0
        blocks += [key_own[step], value_own[step]]
        valid.append(exists)
        blocks += [key_other[step], value_other[step]]
        if step == 0:
            exists = exists & (member == 1)
        elif step == reach:
            exists = exists & (member == 0)
        valid.append(exists)
    sources = len(valid)
    valid = jnp.stack(valid).astype(jnp.int32)

    def kernel(*refs):
        attention_kernel(tokens, heads, head_size, tile, sources, *refs)

    vmem = pl.BlockSpec(memory_space=pltpu.VMEM)
    smem = pl.BlockSpec(memory_space=pltpu.SMEM)
    return pl.pallas_call(
        kernel,
        out_shape=jax.ShapeDtypeStruct((tokens, width), jnp.bfloat16),
        in_specs=[smem, smem] + [vmem] * (3 + len(blocks)),
        out_specs=vmem,
        scratch_shapes=[
            pltpu.VMEM((heads, tile, 1), jnp.float32),
            pltpu.VMEM((heads, tile, 1), jnp.float32),
            pltpu.VMEM((tile, width), jnp.float32),
        ],
        compiler_params=pltpu.CompilerParams(vmem_limit_bytes=50 * 2**20),
        name="attention",
    )(valid, documents, queries, meta, head_gain[None, :], *blocks)


def on_device(
    queries,
    keys,
    values,
    cum_gate,
    documents,
    head_gain,
    out_weight,
    resid,
    norm_gain,
    routes,
    route_weights,
    w_gate,
    w_up,
    w_down,
):
    tokens = queries.shape[0]
    head_normed = attend(queries, keys, values, cum_gate, documents, head_gain)
    tp_count = lax.axis_size("tp")
    local_rows = tokens // tp_count
    regrouped = lax.all_to_all(head_normed, "tp", split_axis=0, concat_axis=1, tiled=True)
    projected = jnp.dot(regrouped, out_weight, preferred_element_type=jnp.float32)
    stream = lax.optimization_barrier((resid.astype(jnp.float32) + projected).astype(jnp.bfloat16))
    widened = stream.astype(jnp.float32)
    mean_wide = jnp.mean(widened * widened, axis=-1, keepdims=True)
    expert_input = (widened * lax.rsqrt(mean_wide + EPS) * norm_gain).astype(jnp.bfloat16)
    top_count = routes.shape[1]
    expert_count = lax.axis_size("sp")
    model_width = stream.shape[1]
    capacity = 2 * top_count * tokens // (tp_count * expert_count)
    flat_routes = routes.reshape(-1)
    route_total = flat_routes.shape[0]
    onehot = (flat_routes[:, None] == jnp.arange(expert_count, dtype=jnp.int32)[None, :]).astype(
        jnp.int32
    )
    ranks = jnp.sum(jnp.cumsum(onehot, axis=0) * onehot, axis=1) - 1
    targets = flat_routes * capacity + ranks
    owners = jnp.arange(route_total, dtype=jnp.int32) // top_count
    slot_owner = jnp.zeros((expert_count * capacity,), jnp.int32).at[targets].set(owners)
    slot_used = jnp.zeros((expert_count * capacity,), jnp.bool_).at[targets].set(True)
    outbound = jnp.where(slot_used[:, None], expert_input[slot_owner], jnp.zeros((), jnp.bfloat16))
    outbound = outbound.reshape(expert_count, capacity, model_width)
    fanned = lax.all_gather(
        lax.all_to_all(outbound, "sp", split_axis=0, concat_axis=0, tiled=True)[:, None],
        "tp",
        axis=1,
        tiled=True,
    )
    flat_rows = fanned.reshape(-1, model_width)
    gate_out = jnp.dot(flat_rows, w_gate[0], preferred_element_type=jnp.float32)
    up_out = jnp.dot(flat_rows, w_up[0], preferred_element_type=jnp.float32)
    hidden = (jax.nn.silu(gate_out) * up_out).astype(jnp.bfloat16)
    partial_value = jnp.dot(hidden, w_down[0], preferred_element_type=jnp.float32)
    partial_value = lax.optimization_barrier(partial_value.astype(jnp.bfloat16)).astype(jnp.float32)
    finish_partial_value = partial_value.reshape(fanned.shape)
    summed = lax.psum_scatter(
        finish_partial_value.astype(jnp.bfloat16), "tp", scatter_dimension=1, tiled=True
    ).astype(jnp.float32)
    returned = lax.all_to_all(
        summed[:, 0].astype(jnp.bfloat16), "sp", split_axis=0, concat_axis=0, tiled=True
    )
    results = returned.reshape(expert_count * capacity, model_width)[targets]
    results = results.reshape(local_rows, top_count, model_width)
    mixed = widened + jnp.sum(route_weights[:, :, None] * results.astype(jnp.float32), axis=1)
    return mixed.astype(jnp.bfloat16)


def solution(mesh):
    in_specs = (
        P("sp", "tp"),
        P("sp", "tp"),
        P("sp", "tp"),
        P("sp", "tp"),
        P("sp"),
        P("tp"),
        P(),
        P(("sp", "tp"), None),
        P(),
        P(("sp", "tp"), None),
        P(("sp", "tp"), None),
        P("sp", None, "tp"),
        P("sp", None, "tp"),
        P("sp", "tp", None),
    )
    out_specs = P(("sp", "tp"), None)
    return jax.shard_map(
        on_device, mesh=mesh, in_specs=in_specs, out_specs=out_specs, check_vma=False
    )
```

```python
import jax
import jax.numpy as jnp
from jax import lax
from jax.experimental import pallas as pl
from jax.experimental.pallas import tpu as pltpu
from jax.sharding import PartitionSpec as P

EPS = 1e-06
LOG2E = 1.4426950408889634
NEG = -1e30


def bf16_parts(x):
    hi = lax.reduce_precision(x, 8, 7)
    rest = x - hi
    mid = lax.reduce_precision(rest, 8, 7)
    low = rest - mid
    return [part.astype(jnp.bfloat16) for part in (hi, mid, low)]


def attention_kernel(tokens, heads, head_size, tile, sources, *refs):
    valid_ref, docs_ref, q_ref, meta_ref, gain_ref = refs[:5]
    kv_refs = refs[5 : 5 + 2 * sources]
    mine_ref, other_ref = refs[5 + 2 * sources : 7 + 2 * sources]
    m_ref, l_ref, acc_ref = refs[7 + 2 * sources :]
    width = heads * head_size
    halves = tokens // width
    rows = tokens // head_size
    score_scale = head_size ** (-0.5) * LOG2E
    lane = lax.broadcasted_iota(jnp.int32, (1, width), 1)
    in_head = [(lane >= h * head_size) & (lane < (h + 1) * head_size) for h in range(heads)]

    def spread(parts):
        full = jnp.broadcast_to(parts[0], (tile, width))
        for h in range(1, heads):
            full = jnp.where(in_head[h], parts[h], full)
        return full

    def q_tile(step, carry):
        row0 = pl.multiple_of(step * tile, tile)
        q = q_ref[pl.ds(row0, tile), :]
        meta = meta_ref[pl.ds(row0, tile), :]
        q_doc = meta[:, heads : heads + 1]
        first_doc = docs_ref[row0].astype(jnp.float32)

        def visit(source):
            k_ref, v_ref = kv_refs[2 * source], kv_refs[2 * source + 1]
            k = k_ref[:tokens, :]
            v = v_ref[...]
            extra = k_ref[tokens:, :].astype(jnp.float32)
            gates = (extra[:rows] + extra[rows : 2 * rows] + extra[2 * rows : 3 * rows]) * LOG2E
            doc_rows = extra[3 * rows : 3 * rows + halves]
            k_doc = jnp.concatenate([doc_rows[j : j + 1] for j in range(halves)], axis=1)
            allowed = k_doc == q_doc
            if source == 0:
                q_pos = row0 + lax.broadcasted_iota(jnp.int32, (tile, tokens), 0)
                k_pos = lax.broadcasted_iota(jnp.int32, (tile, tokens), 1)
                allowed = allowed & (k_pos <= q_pos)
            total = jnp.zeros((tile, width), jnp.float32)
            rescales = []
            for h in range(heads):
                q_h = jnp.where(in_head[h], q, jnp.zeros((), q.dtype))
                s = lax.dot_general(
                    q_h, k, (((1,), (1,)), ((), ())), preferred_element_type=jnp.float32
                )
                gate_row = jnp.concatenate(
                    [gates[h * halves + j : h * halves + j + 1] for j in range(halves)], axis=1
                )
                s = s * score_scale + (meta[:, h : h + 1] * LOG2E - gate_row)
                s = jnp.where(allowed, s, NEG)
                block_max = jnp.max(s, axis=1, keepdims=True)
                if source == 0:
                    new_max = block_max
                else:
                    old_max = m_ref[h]
                    new_max = jnp.maximum(old_max, block_max)
                    rescale = jnp.exp2(old_max - new_max)
                    rescales.append(rescale)
                p = jnp.exp2(s - new_max)
                block_sum = jnp.sum(p, axis=1, keepdims=True)
                m_ref[h] = new_max
                l_ref[h] = block_sum if source == 0 else l_ref[h] * rescale + block_sum
                v_h = jnp.where(in_head[h], v, jnp.zeros((), v.dtype))
                total = total + jnp.dot(
                    p.astype(jnp.bfloat16), v_h, preferred_element_type=jnp.float32
                )
            if source == 0:
                acc_ref[...] = total
            else:
                acc_ref[...] = acc_ref[...] * spread(rescales) + total

        visit(0)
        for source in range(1, sources):
            last_doc = jnp.max(
                kv_refs[2 * source][tokens + 3 * rows : tokens + 3 * rows + halves, :].astype(
                    jnp.float32
                )
            )

            @pl.when((valid_ref[source] > 0) & (last_doc >= first_doc))
            def _():
                visit(source)

        attended = acc_ref[...] / spread([l_ref[h] for h in range(heads)])
        squares = attended * attended
        means = [
            jnp.sum(jnp.where(in_head[h], squares, 0.0), axis=1, keepdims=True) / head_size
            for h in range(heads)
        ]
        scale = spread([lax.rsqrt(mean + EPS) for mean in means])
        normed = (attended * scale * gain_ref[...]).astype(jnp.bfloat16)
        here = pl.ds(pl.multiple_of((step // 2) * tile, tile), tile)

        @pl.when(step % 2 == valid_ref[sources])
        def _():
            mine_ref[here, :] = normed

        @pl.when(step % 2 != valid_ref[sources])
        def _():
            other_ref[here, :] = normed

        return carry

    lax.fori_loop(0, tokens // tile, q_tile, 0)


def attend(queries, keys, values, cum_gate, documents, head_gain):
    tokens, width = queries.shape
    heads = cum_gate.shape[1]
    head_size = width // heads
    n_sp = lax.axis_size("sp")
    place = lax.axis_index("sp")
    tile = tokens // lax.axis_size("tp")

    gate_rows = [part.T.reshape(-1, width) for part in bf16_parts(cum_gate)]
    doc_rows = documents.astype(jnp.bfloat16).reshape(-1, width)
    used = sum(part.shape[0] for part in gate_rows) + doc_rows.shape[0]
    filler = jnp.zeros((-used % 16, width), jnp.bfloat16)
    keys_more = jnp.concatenate([keys, *gate_rows, doc_rows, filler], axis=0)
    meta = jnp.concatenate(
        [
            cum_gate,
            documents.astype(jnp.float32)[:, None],
            jnp.zeros((tokens, 8 - (heads + 1) % 8), jnp.float32),
        ],
        axis=1,
    )

    reach = n_sp // 4
    ahead = [(i, i + 2) for i in range(n_sp - 2)]
    even_up = [(i, i + 1) for i in range(0, n_sp, 2)]
    odd_down = [(i + 1, i) for i in range(0, n_sp, 2)]

    def chain(first):
        own, other = [first], []
        for step in range(reach + 1):
            pairs = even_up if step == 0 else odd_down if step == reach else even_up + odd_down
            if step > 0:
                own.append(lax.ppermute(own[-1], "sp", ahead))
            other.append(lax.ppermute(own[-1], "sp", pairs))
        return own, other

    key_own, key_other = chain(keys_more)
    value_own, value_other = chain(values)
    group, member = place // 2, place % 2
    blocks, valid = [], []
    for step in range(reach + 1):
        exists = group - step >= 0
        blocks += [key_own[step], value_own[step]]
        valid.append(exists)
        blocks += [key_other[step], value_other[step]]
        if step == 0:
            exists = exists & (member == 1)
        elif step == reach:
            exists = exists & (member == 0)
        valid.append(exists)
    sources = len(valid)
    valid = jnp.stack(valid + [lax.axis_index("tp") % 2 == 1]).astype(jnp.int32)

    def kernel(*refs):
        attention_kernel(tokens, heads, head_size, tile, sources, *refs)

    vmem = pl.BlockSpec(memory_space=pltpu.VMEM)
    smem = pl.BlockSpec(memory_space=pltpu.SMEM)
    return pl.pallas_call(
        kernel,
        out_shape=[jax.ShapeDtypeStruct((tokens // 2, width), jnp.bfloat16)] * 2,
        in_specs=[smem, smem] + [vmem] * (3 + len(blocks)),
        out_specs=[vmem, vmem],
        scratch_shapes=[
            pltpu.VMEM((heads, tile, 1), jnp.float32),
            pltpu.VMEM((heads, tile, 1), jnp.float32),
            pltpu.VMEM((tile, width), jnp.float32),
        ],
        compiler_params=pltpu.CompilerParams(vmem_limit_bytes=50 * 2**20),
        name="attention",
    )(valid, documents, queries, meta, head_gain[None, :], *blocks)


def swap(x, axis, bits):
    return lax.ppermute(x, axis, [(i, i ^ bits) for i in range(lax.axis_size(axis))])


def project_kernel(experts, capacity, n_tp, *refs):
    blocks = n_tp // 2
    place_ref = refs[0]
    pieces = refs[1 : 1 + n_tp]
    weight_ref = refs[1 + n_tp]
    resids = refs[2 + n_tp : 2 + n_tp + blocks]
    routes = refs[2 + n_tp + blocks : 2 + n_tp + 2 * blocks]
    gain_ref = refs[2 + n_tp + 2 * blocks]
    outs = refs[3 + n_tp + 2 * blocks : 3 + n_tp + 2 * blocks + experts]
    stream_ref, wide_ref, packed_ref, slot_ref, pick_ref = refs[3 + n_tp + 2 * blocks + experts :]
    rows, width = resids[0].shape
    part = pieces[0].shape[1]
    place, spot = place_ref[0], place_ref[1]
    across = spot // 2
    n_tile = 512

    inputs = [
        jnp.concatenate(
            [
                piece[pl.ds(pl.multiple_of((across ^ j) * rows, rows), rows), :]
                for j in range(blocks)
            ],
            axis=0,
        )
        for piece in pieces
    ]
    total = jnp.zeros((blocks * rows, 1), jnp.float32)
    for n in range(width // n_tile):
        cols = slice(n * n_tile, (n + 1) * n_tile)
        projected = jnp.zeros((blocks * rows, n_tile), jnp.float32)
        for k in range(n_tp):
            from_row = pl.multiple_of((spot ^ k) * part, part)
            projected = projected + jnp.dot(
                inputs[k],
                weight_ref[pl.ds(from_row, part), cols],
                preferred_element_type=jnp.float32,
            )
        resid = jnp.concatenate([resid_ref[:, cols] for resid_ref in resids], axis=0)
        stream = (resid.astype(jnp.float32) + projected).astype(jnp.bfloat16)
        stream_ref[:, cols] = stream[:rows]
        wide = stream.astype(jnp.float32)
        wide_ref[:, cols] = wide
        total = total + jnp.sum(wide * wide, axis=1, keepdims=True)
    scale = lax.rsqrt(total / width + EPS)

    before = (
        lax.broadcasted_iota(jnp.int32, (rows, rows), 0)
        < lax.broadcasted_iota(jnp.int32, (rows, rows), 1)
    ).astype(jnp.bfloat16)
    expert_ids = lax.broadcasted_iota(jnp.int32, (experts, rows), 0).astype(jnp.float32)
    for j in range(blocks):
        chosen = jnp.zeros((experts, rows), jnp.float32)
        for route in range(2):
            chosen = chosen + (routes[j][route : route + 1, :] == expert_ids).astype(jnp.float32)
        ranks = jnp.dot(chosen.astype(jnp.bfloat16), before, preferred_element_type=jnp.float32)
        slot_ref[j] = jnp.where(chosen > 0.0, ranks, -1.0)
    slot_ids = lax.broadcasted_iota(jnp.int32, (capacity, rows), 0).astype(jnp.float32)
    for k in range(experts):
        for j in range(blocks):
            row_of = slot_ref[j, pl.ds(place ^ k, 1), :]
            first = (k * blocks + j) * capacity
            for i in range(blocks):
                pick = (slot_ids == row_of) if i == j else jnp.zeros((capacity, rows), jnp.bool_)
                pick_ref[first : first + capacity, i * rows : (i + 1) * rows] = pick.astype(
                    jnp.float32
                ).astype(jnp.bfloat16)
    each = blocks * capacity
    for n in range(width // n_tile):
        cols = slice(n * n_tile, (n + 1) * n_tile)
        packed_ref[...] = (wide_ref[:, cols] * scale * gain_ref[:, cols]).astype(jnp.bfloat16)
        picked = jnp.dot(
            pick_ref[...], packed_ref[...], preferred_element_type=jnp.float32
        ).astype(jnp.bfloat16)
        for k in range(experts):
            outs[k][:, cols] = picked[k * each : (k + 1) * each]


def expert_kernel(members, *refs):
    inputs = refs[: 2 * members]
    gate_ref, up_ref, down_hbm = refs[2 * members : 2 * members + 3]
    mine_ref, other_ref, x_ref, hidden_ref, down_ref, sem = refs[2 * members + 3 :]
    each = inputs[0].shape[0]
    step, steps = pl.program_id(0), hidden_ref.shape[0]
    fetch = pltpu.make_async_copy(down_hbm, down_ref, sem)

    @pl.when(step == 0)
    def _():
        fetch.start()
        for i, ref in enumerate(inputs):
            x_ref[i * each : (i + 1) * each, :] = ref[...]

    both = jnp.concatenate([gate_ref[...], up_ref[...]], axis=1)
    product = jnp.dot(x_ref[...], both, preferred_element_type=jnp.float32)
    half = product.shape[1] // 2
    gate, up = product[:, :half], product[:, half:]
    hidden_ref[step] = (gate * (1.0 / (1.0 + jnp.exp(-gate))) * up).astype(jnp.bfloat16)

    @pl.when(step == steps - 1)
    def _():
        fetch.wait()
        hidden = jnp.concatenate([hidden_ref[i] for i in range(steps)], axis=1)
        n_tile = 512
        for n in range(down_ref.shape[1] // n_tile):
            cols = slice(n * n_tile, (n + 1) * n_tile)
            out = jnp.dot(
                hidden, down_ref[:, cols], preferred_element_type=jnp.float32
            ).astype(jnp.bfloat16)
            mine_ref[:, cols] = out[: members * each]
            other_ref[:, cols] = out[members * each :]


def combine_kernel(experts, place_ref, stream_ref, routes_ref, weights_ref, *refs):
    outs = refs[:experts]
    mixed_ref, stack_ref = refs[experts:]
    rows, width = stream_ref.shape
    capacity = outs[0].shape[0]
    for k in range(experts):
        stack_ref[k * capacity : (k + 1) * capacity, :] = outs[k][...]
    expert_ids = lax.broadcasted_iota(jnp.int32, (rows, experts), 1)
    named = [
        (routes_ref[:, route : route + 1] == expert_ids).astype(jnp.float32) for route in range(2)
    ]
    before = (
        lax.broadcasted_iota(jnp.int32, (rows, rows), 1)
        < lax.broadcasted_iota(jnp.int32, (rows, rows), 0)
    ).astype(jnp.bfloat16)
    ranks = jnp.dot(
        before, (named[0] + named[1]).astype(jnp.bfloat16), preferred_element_type=jnp.float32
    )
    slot_ids = lax.broadcasted_iota(jnp.int32, (rows, experts * capacity), 1)
    picks = []
    for route in range(2):
        rank = jnp.sum(named[route] * ranks, axis=1, keepdims=True).astype(jnp.int32)
        target = (routes_ref[:, route : route + 1] ^ place_ref[0]) * capacity + rank
        picks.append((slot_ids == target).astype(jnp.float32).astype(jnp.bfloat16))
    n_tile = 512
    for n in range(width // n_tile):
        cols = slice(n * n_tile, (n + 1) * n_tile)
        mixed = stream_ref[:, cols].astype(jnp.float32)
        for route in range(2):
            result = jnp.dot(picks[route], stack_ref[:, cols], preferred_element_type=jnp.float32)
            mixed = mixed + weights_ref[:, route : route + 1] * result
        mixed_ref[:, cols] = mixed.astype(jnp.bfloat16)


def on_device(
    queries,
    keys,
    values,
    cum_gate,
    documents,
    head_gain,
    out_weight,
    resid,
    norm_gain,
    routes,
    route_weights,
    w_gate,
    w_up,
    w_down,
):
    tokens = queries.shape[0]
    n_sp, n_tp = lax.axis_size("sp"), lax.axis_size("tp")
    place, spot = lax.axis_index("sp"), lax.axis_index("tp")
    blocks = n_tp // 2
    local_rows, model_width = resid.shape
    capacity = 2 * routes.shape[1] * tokens // (n_tp * n_sp)
    each = blocks * capacity
    vmem = pl.BlockSpec(memory_space=pltpu.VMEM)
    smem = pl.BlockSpec(memory_space=pltpu.SMEM)
    places = jnp.stack([place, spot]).astype(jnp.int32)

    route_rows = jnp.concatenate(
        [routes.T.astype(jnp.float32), jnp.zeros((8 - routes.shape[1], local_rows), jnp.float32)],
        axis=0,
    )
    resids = [resid] + [swap(resid, "tp", 2 * j) for j in range(1, blocks)]
    route_blocks = [route_rows] + [swap(route_rows, "tp", 2 * j) for j in range(1, blocks)]

    mine, other = attend(queries, keys, values, cum_gate, documents, head_gain)
    pieces = [mine] + [swap(other if k % 2 else mine, "tp", k) for k in range(1, n_tp)]

    def project(*refs):
        project_kernel(n_sp, capacity, n_tp, *refs)

    *outbound, stream = pl.pallas_call(
        project,
        out_shape=[jax.ShapeDtypeStruct((each, model_width), jnp.bfloat16)] * n_sp
        + [jax.ShapeDtypeStruct((local_rows, model_width), jnp.bfloat16)],
        in_specs=[smem] + [vmem] * (n_tp + 2 + 2 * blocks),
        out_specs=[vmem] * (n_sp + 1),
        scratch_shapes=[
            pltpu.VMEM((blocks * local_rows, model_width), jnp.float32),
            pltpu.VMEM((blocks * local_rows, 512), jnp.bfloat16),
            pltpu.VMEM((blocks, n_sp, local_rows), jnp.float32),
            pltpu.VMEM((n_sp * each, blocks * local_rows), jnp.bfloat16),
        ],
        compiler_params=pltpu.CompilerParams(vmem_limit_bytes=40 * 2**20),
        name="project",
    )(places, *pieces, out_weight, *resids, *route_blocks, norm_gain[None, :])

    members = max(1, n_sp * each // (4 * each))
    hidden_width = w_gate.shape[2]
    h_tile = 128
    order = [k ^ (k >> 1) for k in range(n_sp)]
    arrived = {k: swap(outbound[k], "sp", k) if k else outbound[k] for k in order}
    returned = {}
    for start in range(0, n_sp, members):
        group = order[start : start + members]
        shared = [swap(arrived[k], "tp", 1) for k in group]
        rows = 2 * members * each

        def expert(*refs):
            expert_kernel(members, *refs)

        full = pl.BlockSpec((each, model_width), lambda f: (0, 0))
        part_mine, part_other = pl.pallas_call(
            expert,
            grid=(hidden_width // h_tile,),
            out_shape=[jax.ShapeDtypeStruct((members * each, model_width), jnp.bfloat16)] * 2,
            in_specs=[full] * (2 * members)
            + [pl.BlockSpec((model_width, h_tile), lambda f: (0, f))] * 2
            + [pl.BlockSpec(memory_space=pl.ANY)],
            out_specs=[pl.BlockSpec((members * each, model_width), lambda f: (0, 0))] * 2,
            scratch_shapes=[
                pltpu.VMEM((rows, model_width), jnp.bfloat16),
                pltpu.VMEM((hidden_width // h_tile, rows, h_tile), jnp.bfloat16),
                pltpu.VMEM((hidden_width, model_width), jnp.bfloat16),
                pltpu.SemaphoreType.DMA,
            ],
            compiler_params=pltpu.CompilerParams(
                dimension_semantics=("arbitrary",), vmem_limit_bytes=40 * 2**20
            ),
            cost_estimate=pl.CostEstimate(
                flops=6 * rows * model_width * hidden_width,
                transcendentals=rows * hidden_width,
                bytes_accessed=6 * model_width * hidden_width + 4 * rows * model_width,
            ),
            name="expert",
        )(*[arrived[k] for k in group], *shared, w_gate[0], w_up[0], w_down[0])
        added = swap(part_other, "tp", 1)
        shape = (members, blocks, capacity, model_width)
        part_mine, added = part_mine.reshape(shape), added.reshape(shape)

        def summed(i, j):
            return part_mine[i, j].astype(jnp.float32) + added[i, j].astype(jnp.float32)

        for i, k in enumerate(group):
            result = summed(i, 0)
            for j in range(1, blocks):
                sent = swap(summed(i, j).astype(jnp.bfloat16), "tp", 2 * j)
                result = result + sent.astype(jnp.float32)
            result = result.astype(jnp.bfloat16)
            returned[k] = swap(result, "sp", k) if k else result

    def combine(*refs):
        combine_kernel(n_sp, *refs)

    return pl.pallas_call(
        combine,
        out_shape=jax.ShapeDtypeStruct((local_rows, model_width), jnp.bfloat16),
        in_specs=[smem] + [vmem] * (3 + n_sp),
        out_specs=vmem,
        scratch_shapes=[pltpu.VMEM((n_sp * capacity, model_width), jnp.bfloat16)],
        compiler_params=pltpu.CompilerParams(vmem_limit_bytes=24 * 2**20),
        name="combine",
    )(places, stream, routes, route_weights, *[returned[k] for k in range(n_sp)])


def solution(mesh):
    in_specs = (
        P("sp", "tp"),
        P("sp", "tp"),
        P("sp", "tp"),
        P("sp", "tp"),
        P("sp"),
        P("tp"),
        P(),
        P(("sp", "tp"), None),
        P(),
        P(("sp", "tp"), None),
        P(("sp", "tp"), None),
        P("sp", None, "tp"),
        P("sp", None, "tp"),
        P("sp", "tp", None),
    )
    out_specs = P(("sp", "tp"), None)
    return jax.shard_map(
        on_device, mesh=mesh, in_specs=in_specs, out_specs=out_specs, check_vma=False
    )
```

```python
import jax
import jax.numpy as jnp
from jax import lax
from jax.experimental import pallas as pl
from jax.experimental.pallas import tpu as pltpu
from jax.sharding import PartitionSpec as P

EPS = 1e-06
LOG2E = 1.4426950408889634
NEG = -1e30


def bf16_parts(x):
    hi = lax.reduce_precision(x, 8, 7)
    rest = x - hi
    mid = lax.reduce_precision(rest, 8, 7)
    low = rest - mid
    return [part.astype(jnp.bfloat16) for part in (hi, mid, low)]


def attention_kernel(tokens, heads, head_size, tile, sources, *refs):
    valid_ref, docs_ref, q_ref, meta_ref, gain_ref = refs[:5]
    kv_refs = refs[5 : 5 + 2 * sources]
    mine_ref, other_ref = refs[5 + 2 * sources : 7 + 2 * sources]
    m_ref, l_ref, acc_ref = refs[7 + 2 * sources :]
    width = heads * head_size
    halves = tokens // width
    rows = tokens // head_size
    score_scale = head_size ** (-0.5) * LOG2E
    lane = lax.broadcasted_iota(jnp.int32, (1, width), 1)
    in_head = [(lane >= h * head_size) & (lane < (h + 1) * head_size) for h in range(heads)]

    def spread(parts):
        full = jnp.broadcast_to(parts[0], (tile, width))
        for h in range(1, heads):
            full = jnp.where(in_head[h], parts[h], full)
        return full

    def q_tile(step, carry):
        row0 = pl.multiple_of(step * tile, tile)
        q = q_ref[pl.ds(row0, tile), :]
        meta = meta_ref[pl.ds(row0, tile), :]
        q_doc = meta[:, heads : heads + 1]
        first_doc = docs_ref[row0].astype(jnp.float32)

        def visit(source):
            k_ref, v_ref = kv_refs[2 * source], kv_refs[2 * source + 1]
            k = k_ref[:tokens, :]
            v = v_ref[...]
            extra = k_ref[tokens:, :].astype(jnp.float32)
            gates = (extra[:rows] + extra[rows : 2 * rows] + extra[2 * rows : 3 * rows]) * LOG2E
            doc_rows = extra[3 * rows : 3 * rows + halves]
            k_doc = jnp.concatenate([doc_rows[j : j + 1] for j in range(halves)], axis=1)
            allowed = k_doc == q_doc
            if source == 0:
                q_pos = row0 + lax.broadcasted_iota(jnp.int32, (tile, tokens), 0)
                k_pos = lax.broadcasted_iota(jnp.int32, (tile, tokens), 1)
                allowed = allowed & (k_pos <= q_pos)
            total = jnp.zeros((tile, width), jnp.float32)
            rescales = []
            for h in range(heads):
                q_h = jnp.where(in_head[h], q, jnp.zeros((), q.dtype))
                s = lax.dot_general(
                    q_h, k, (((1,), (1,)), ((), ())), preferred_element_type=jnp.float32
                )
                gate_row = jnp.concatenate(
                    [gates[h * halves + j : h * halves + j + 1] for j in range(halves)], axis=1
                )
                s = s * score_scale + (meta[:, h : h + 1] * LOG2E - gate_row)
                s = jnp.where(allowed, s, NEG)
                block_max = jnp.max(s, axis=1, keepdims=True)
                if source == 0:
                    new_max = block_max
                else:
                    old_max = m_ref[h]
                    new_max = jnp.maximum(old_max, block_max)
                    rescale = jnp.exp2(old_max - new_max)
                    rescales.append(rescale)
                p = jnp.exp2(s - new_max)
                block_sum = jnp.sum(p, axis=1, keepdims=True)
                m_ref[h] = new_max
                l_ref[h] = block_sum if source == 0 else l_ref[h] * rescale + block_sum
                v_h = jnp.where(in_head[h], v, jnp.zeros((), v.dtype))
                total = total + jnp.dot(
                    p.astype(jnp.bfloat16), v_h, preferred_element_type=jnp.float32
                )
            if source == 0:
                acc_ref[...] = total
            else:
                acc_ref[...] = acc_ref[...] * spread(rescales) + total

        visit(0)
        for source in range(1, sources):
            last_doc = jnp.max(
                kv_refs[2 * source][tokens + 3 * rows : tokens + 3 * rows + halves, :].astype(
                    jnp.float32
                )
            )

            @pl.when((valid_ref[source] > 0) & (last_doc >= first_doc))
            def _():
                visit(source)

        attended = acc_ref[...] / spread([l_ref[h] for h in range(heads)])
        squares = attended * attended
        means = [
            jnp.sum(jnp.where(in_head[h], squares, 0.0), axis=1, keepdims=True) / head_size
            for h in range(heads)
        ]
        scale = spread([lax.rsqrt(mean + EPS) for mean in means])
        normed = (attended * scale * gain_ref[...]).astype(jnp.bfloat16)
        here = pl.ds(pl.multiple_of((step // 2) * tile, tile), tile)

        @pl.when(step % 2 == valid_ref[sources])
        def _():
            mine_ref[here, :] = normed

        @pl.when(step % 2 != valid_ref[sources])
        def _():
            other_ref[here, :] = normed

        return carry

    lax.fori_loop(0, tokens // tile, q_tile, 0)


def attend(queries, keys, values, cum_gate, documents, head_gain):
    tokens, width = queries.shape
    heads = cum_gate.shape[1]
    head_size = width // heads
    n_sp = lax.axis_size("sp")
    place = lax.axis_index("sp")
    tile = tokens // lax.axis_size("tp")

    gate_rows = [part.T.reshape(-1, width) for part in bf16_parts(cum_gate)]
    doc_rows = documents.astype(jnp.bfloat16).reshape(-1, width)
    used = sum(part.shape[0] for part in gate_rows) + doc_rows.shape[0]
    filler = jnp.zeros((-used % 16, width), jnp.bfloat16)
    keys_more = jnp.concatenate([keys, *gate_rows, doc_rows, filler], axis=0)
    meta = jnp.concatenate(
        [
            cum_gate,
            documents.astype(jnp.float32)[:, None],
            jnp.zeros((tokens, 8 - (heads + 1) % 8), jnp.float32),
        ],
        axis=1,
    )

    reach = n_sp // 4
    ahead = [(i, i + 2) for i in range(n_sp - 2)]
    even_up = [(i, i + 1) for i in range(0, n_sp, 2)]
    odd_down = [(i + 1, i) for i in range(0, n_sp, 2)]

    def chain(first):
        own, other = [first], []
        for step in range(reach + 1):
            pairs = even_up if step == 0 else odd_down if step == reach else even_up + odd_down
            if step > 0:
                own.append(lax.ppermute(own[-1], "sp", ahead))
            other.append(lax.ppermute(own[-1], "sp", pairs))
        return own, other

    key_own, key_other = chain(keys_more)
    value_own, value_other = chain(values)
    group, member = place // 2, place % 2
    blocks, valid = [], []
    for step in range(reach + 1):
        exists = group - step >= 0
        blocks += [key_own[step], value_own[step]]
        valid.append(exists)
        blocks += [key_other[step], value_other[step]]
        if step == 0:
            exists = exists & (member == 1)
        elif step == reach:
            exists = exists & (member == 0)
        valid.append(exists)
    sources = len(valid)
    valid = jnp.stack(valid + [lax.axis_index("tp") % 2 == 1]).astype(jnp.int32)

    def kernel(*refs):
        attention_kernel(tokens, heads, head_size, tile, sources, *refs)

    vmem = pl.BlockSpec(memory_space=pltpu.VMEM)
    smem = pl.BlockSpec(memory_space=pltpu.SMEM)
    return pl.pallas_call(
        kernel,
        out_shape=[jax.ShapeDtypeStruct((tokens // 2, width), jnp.bfloat16)] * 2,
        in_specs=[smem, smem] + [vmem] * (3 + len(blocks)),
        out_specs=[vmem, vmem],
        scratch_shapes=[
            pltpu.VMEM((heads, tile, 1), jnp.float32),
            pltpu.VMEM((heads, tile, 1), jnp.float32),
            pltpu.VMEM((tile, width), jnp.float32),
        ],
        compiler_params=pltpu.CompilerParams(vmem_limit_bytes=50 * 2**20),
        name="attention",
    )(valid, documents, queries, meta, head_gain[None, :], *blocks)


def swap(x, axis, bits):
    return lax.ppermute(x, axis, [(i, i ^ bits) for i in range(lax.axis_size(axis))])


def far_places(n_sp):
    return [k for k in range(n_sp) if k & (n_sp // 2) and not k & (n_sp // 4)]


def expert_groups(n_sp):
    far = far_places(n_sp)
    near = [k ^ (k >> 1) for k in range(n_sp)]
    near = [k for k in near if k not in far]
    size = n_sp // 4
    return [near[:size], near[size : 2 * size], far[::-1], near[2 * size :]]


def project_kernel(experts, capacity, n_tp, far, *refs):
    blocks = n_tp // 2
    place_ref = refs[0]
    pieces = refs[1 : 1 + n_tp]
    weight_ref = refs[1 + n_tp]
    resids = refs[2 + n_tp : 2 + n_tp + blocks]
    routes = refs[2 + n_tp + blocks : 2 + n_tp + 2 * blocks]
    gain_ref = refs[2 + n_tp + 2 * blocks]
    outs = refs[3 + n_tp + 2 * blocks : 3 + n_tp + 2 * blocks + experts]
    stream_ref, wide_ref, packed_ref, slot_ref, pick_ref = refs[3 + n_tp + 2 * blocks + experts :]
    rows, width = resids[0].shape
    part = pieces[0].shape[1]
    place, spot = place_ref[0], place_ref[1]
    across = spot // 2
    n_tile = 512

    inputs = [
        jnp.concatenate(
            [
                piece[pl.ds(pl.multiple_of((across ^ j) * rows, rows), rows), :]
                for j in range(blocks)
            ],
            axis=0,
        )
        for piece in pieces
    ]
    total = jnp.zeros((blocks * rows, 1), jnp.float32)
    for n in range(width // n_tile):
        cols = slice(n * n_tile, (n + 1) * n_tile)
        projected = jnp.zeros((blocks * rows, n_tile), jnp.float32)
        for k in range(n_tp):
            from_row = pl.multiple_of((spot ^ k) * part, part)
            projected = projected + jnp.dot(
                inputs[k],
                weight_ref[pl.ds(from_row, part), cols],
                preferred_element_type=jnp.float32,
            )
        resid = jnp.concatenate([resid_ref[:, cols] for resid_ref in resids], axis=0)
        stream = (resid.astype(jnp.float32) + projected).astype(jnp.bfloat16)
        stream_ref[:, cols] = stream[:rows]
        wide = stream.astype(jnp.float32)
        wide_ref[:, cols] = wide
        total = total + jnp.sum(wide * wide, axis=1, keepdims=True)
    scale = lax.rsqrt(total / width + EPS)

    before = (
        lax.broadcasted_iota(jnp.int32, (rows, rows), 0)
        < lax.broadcasted_iota(jnp.int32, (rows, rows), 1)
    ).astype(jnp.bfloat16)
    expert_ids = lax.broadcasted_iota(jnp.int32, (experts, rows), 0).astype(jnp.float32)
    for j in range(blocks):
        chosen = jnp.zeros((experts, rows), jnp.float32)
        for route in range(2):
            chosen = chosen + (routes[j][route : route + 1, :] == expert_ids).astype(jnp.float32)
        ranks = jnp.dot(chosen.astype(jnp.bfloat16), before, preferred_element_type=jnp.float32)
        slot_ref[j] = jnp.where(chosen > 0.0, ranks, -1.0)
    slot_ids = lax.broadcasted_iota(jnp.int32, (capacity, rows), 0).astype(jnp.float32)
    first, spans = 0, []
    for k in range(experts):
        spans.append(first)
        for j in range(1 if k in far else blocks):
            row_of = slot_ref[j, pl.ds(place ^ k, 1), :]
            for i in range(blocks):
                pick = (slot_ids == row_of) if i == j else jnp.zeros((capacity, rows), jnp.bool_)
                pick_ref[first : first + capacity, i * rows : (i + 1) * rows] = pick.astype(
                    jnp.float32
                ).astype(jnp.bfloat16)
            first += capacity
    spans.append(first)
    for n in range(width // n_tile):
        cols = slice(n * n_tile, (n + 1) * n_tile)
        packed_ref[...] = (wide_ref[:, cols] * scale * gain_ref[:, cols]).astype(jnp.bfloat16)
        picked = jnp.dot(
            pick_ref[...], packed_ref[...], preferred_element_type=jnp.float32
        ).astype(jnp.bfloat16)
        for k in range(experts):
            outs[k][:, cols] = picked[spans[k] : spans[k + 1]]


def expert_kernel(count, *refs):
    inputs = refs[:count]
    gate_ref, up_ref, down_hbm = refs[count : count + 3]
    mine_ref, other_ref, x_ref, hidden_ref, down_ref, sem = refs[count + 3 :]
    mine_rows = mine_ref.shape[0]
    step, steps = pl.program_id(0), hidden_ref.shape[0]
    fetch = pltpu.make_async_copy(down_hbm, down_ref, sem)

    @pl.when(step == 0)
    def _():
        fetch.start()
        row = 0
        for ref in inputs:
            x_ref[row : row + ref.shape[0], :] = ref[...]
            row += ref.shape[0]

    both = jnp.concatenate([gate_ref[...], up_ref[...]], axis=1)
    product = jnp.dot(x_ref[...], both, preferred_element_type=jnp.float32)
    half = product.shape[1] // 2
    gate, up = product[:, :half], product[:, half:]
    hidden_ref[step] = (gate * (1.0 / (1.0 + jnp.exp(-gate))) * up).astype(jnp.bfloat16)

    @pl.when(step == steps - 1)
    def _():
        fetch.wait()
        hidden = jnp.concatenate([hidden_ref[i] for i in range(steps)], axis=1)
        n_tile = 512
        for n in range(down_ref.shape[1] // n_tile):
            cols = slice(n * n_tile, (n + 1) * n_tile)
            out = jnp.dot(
                hidden, down_ref[:, cols], preferred_element_type=jnp.float32
            ).astype(jnp.bfloat16)
            mine_ref[:, cols] = out[:mine_rows]
            other_ref[:, cols] = out[mine_rows:]


def combine_kernel(experts, place_ref, stream_ref, routes_ref, weights_ref, *refs):
    outs = refs[:experts]
    mixed_ref, stack_ref = refs[experts:]
    rows, width = stream_ref.shape
    capacity = outs[0].shape[0]
    for k in range(experts):
        stack_ref[k * capacity : (k + 1) * capacity, :] = outs[k][...]
    expert_ids = lax.broadcasted_iota(jnp.int32, (rows, experts), 1)
    named = [
        (routes_ref[:, route : route + 1] == expert_ids).astype(jnp.float32) for route in range(2)
    ]
    before = (
        lax.broadcasted_iota(jnp.int32, (rows, rows), 1)
        < lax.broadcasted_iota(jnp.int32, (rows, rows), 0)
    ).astype(jnp.bfloat16)
    ranks = jnp.dot(
        before, (named[0] + named[1]).astype(jnp.bfloat16), preferred_element_type=jnp.float32
    )
    slot_ids = lax.broadcasted_iota(jnp.int32, (rows, experts * capacity), 1)
    picks = []
    for route in range(2):
        rank = jnp.sum(named[route] * ranks, axis=1, keepdims=True).astype(jnp.int32)
        target = (routes_ref[:, route : route + 1] ^ place_ref[0]) * capacity + rank
        picks.append((slot_ids == target).astype(jnp.float32).astype(jnp.bfloat16))
    n_tile = 512
    for n in range(width // n_tile):
        cols = slice(n * n_tile, (n + 1) * n_tile)
        mixed = stream_ref[:, cols].astype(jnp.float32)
        for route in range(2):
            result = jnp.dot(picks[route], stack_ref[:, cols], preferred_element_type=jnp.float32)
            mixed = mixed + weights_ref[:, route : route + 1] * result
        mixed_ref[:, cols] = mixed.astype(jnp.bfloat16)


def on_device(
    queries,
    keys,
    values,
    cum_gate,
    documents,
    head_gain,
    out_weight,
    resid,
    norm_gain,
    routes,
    route_weights,
    w_gate,
    w_up,
    w_down,
):
    tokens = queries.shape[0]
    n_sp, n_tp = lax.axis_size("sp"), lax.axis_size("tp")
    place, spot = lax.axis_index("sp"), lax.axis_index("tp")
    blocks = n_tp // 2
    local_rows, model_width = resid.shape
    capacity = 2 * routes.shape[1] * tokens // (n_tp * n_sp)
    each = blocks * capacity
    vmem = pl.BlockSpec(memory_space=pltpu.VMEM)
    smem = pl.BlockSpec(memory_space=pltpu.SMEM)
    places = jnp.stack([place, spot]).astype(jnp.int32)

    route_rows = jnp.concatenate(
        [routes.T.astype(jnp.float32), jnp.zeros((8 - routes.shape[1], local_rows), jnp.float32)],
        axis=0,
    )
    resids = [resid] + [swap(resid, "tp", 2 * j) for j in range(1, blocks)]
    route_blocks = [route_rows] + [swap(route_rows, "tp", 2 * j) for j in range(1, blocks)]

    mine, other = attend(queries, keys, values, cum_gate, documents, head_gain)
    pieces = [mine] + [swap(other if k % 2 else mine, "tp", k) for k in range(1, n_tp)]

    far = far_places(n_sp)
    counts = [capacity if k in far else each for k in range(n_sp)]

    def project(*refs):
        project_kernel(n_sp, capacity, n_tp, far, *refs)

    *outbound, stream = pl.pallas_call(
        project,
        out_shape=[jax.ShapeDtypeStruct((count, model_width), jnp.bfloat16) for count in counts]
        + [jax.ShapeDtypeStruct((local_rows, model_width), jnp.bfloat16)],
        in_specs=[smem] + [vmem] * (n_tp + 2 + 2 * blocks),
        out_specs=[vmem] * (n_sp + 1),
        scratch_shapes=[
            pltpu.VMEM((blocks * local_rows, model_width), jnp.float32),
            pltpu.VMEM((blocks * local_rows, 512), jnp.bfloat16),
            pltpu.VMEM((blocks, n_sp, local_rows), jnp.float32),
            pltpu.VMEM((sum(counts), blocks * local_rows), jnp.bfloat16),
        ],
        compiler_params=pltpu.CompilerParams(vmem_limit_bytes=40 * 2**20),
        name="project",
    )(places, *pieces, out_weight, *resids, *route_blocks, norm_gain[None, :])

    def hop(x, k):
        if k == 0:
            return x
        if k in far and k % 2:
            low, step = k % (n_sp // 2), n_sp // 4
            x = lax.ppermute(x, "sp", [(i, ((i ^ low) - step) % n_sp) for i in range(n_sp)])
            return lax.ppermute(x, "sp", [(i, (i - step) % n_sp) for i in range(n_sp)])
        return swap(x, "sp", k)

    groups = expert_groups(n_sp)
    members = len(groups[0])
    hidden_width = w_gate.shape[2]
    h_tile = 128
    rows = 2 * members * each
    arrived = {k: hop(outbound[k], k) for group in groups for k in group}
    returned = {}
    for group in groups:
        inputs = []
        for k in group:
            inputs.append(arrived[k])
            if k in far:
                inputs += [swap(arrived[k], "tp", 2 * j) for j in range(1, blocks)]
        inputs += [swap(x, "tp", 1) for x in inputs]

        def expert(*refs):
            expert_kernel(len(inputs), *refs)

        part_mine, part_other = pl.pallas_call(
            expert,
            grid=(hidden_width // h_tile,),
            out_shape=[jax.ShapeDtypeStruct((members * each, model_width), jnp.bfloat16)] * 2,
            in_specs=[pl.BlockSpec(x.shape, lambda f: (0, 0)) for x in inputs]
            + [pl.BlockSpec((model_width, h_tile), lambda f: (0, f))] * 2
            + [pl.BlockSpec(memory_space=pl.ANY)],
            out_specs=[pl.BlockSpec((members * each, model_width), lambda f: (0, 0))] * 2,
            scratch_shapes=[
                pltpu.VMEM((rows, model_width), jnp.bfloat16),
                pltpu.VMEM((hidden_width // h_tile, rows, h_tile), jnp.bfloat16),
                pltpu.VMEM((hidden_width, model_width), jnp.bfloat16),
                pltpu.SemaphoreType.DMA,
            ],
            compiler_params=pltpu.CompilerParams(
                dimension_semantics=("arbitrary",), vmem_limit_bytes=40 * 2**20
            ),
            cost_estimate=pl.CostEstimate(
                flops=6 * rows * model_width * hidden_width,
                transcendentals=rows * hidden_width,
                bytes_accessed=6 * model_width * hidden_width + 4 * rows * model_width,
            ),
            name="expert",
        )(*inputs, w_gate[0], w_up[0], w_down[0])
        added = swap(part_other, "tp", 1)
        shape = (members, blocks, capacity, model_width)
        part_mine, added = part_mine.reshape(shape), added.reshape(shape)

        def summed(j):
            return part_mine[:, j].astype(jnp.float32) + added[:, j].astype(jnp.float32)

        result = summed(0)
        for j in range(1, blocks):
            sent = swap(summed(j).astype(jnp.bfloat16), "tp", 2 * j)
            result = result + sent.astype(jnp.float32)
        result = result.astype(jnp.bfloat16)
        for i, k in enumerate(group):
            returned[k] = hop(result[i], k)

    def combine(*refs):
        combine_kernel(n_sp, *refs)

    return pl.pallas_call(
        combine,
        out_shape=jax.ShapeDtypeStruct((local_rows, model_width), jnp.bfloat16),
        in_specs=[smem] + [vmem] * (3 + n_sp),
        out_specs=vmem,
        scratch_shapes=[pltpu.VMEM((n_sp * capacity, model_width), jnp.bfloat16)],
        compiler_params=pltpu.CompilerParams(vmem_limit_bytes=24 * 2**20),
        name="combine",
    )(places, stream, routes, route_weights, *[returned[k] for k in range(n_sp)])


def solution(mesh):
    in_specs = (
        P("sp", "tp"),
        P("sp", "tp"),
        P("sp", "tp"),
        P("sp", "tp"),
        P("sp"),
        P("tp"),
        P(),
        P(("sp", "tp"), None),
        P(),
        P(("sp", "tp"), None),
        P(("sp", "tp"), None),
        P("sp", None, "tp"),
        P("sp", None, "tp"),
        P("sp", "tp", None),
    )
    out_specs = P(("sp", "tp"), None)


    return jax.shard_map(on_device, mesh=mesh, in_specs=in_specs, out_specs=out_specs, check_vma=False)
```

```python
import jax
import jax.numpy as jnp
from jax import lax
from jax.experimental import pallas as pl
from jax.experimental.pallas import tpu as pltpu
from jax.sharding import PartitionSpec as P

EPS = 1e-06
LOG2E = 1.4426950408889634
NEG = -1e30


def bf16_parts(x):
    hi = lax.reduce_precision(x, 8, 7)
    rest = x - hi
    mid = lax.reduce_precision(rest, 8, 7)
    low = rest - mid
    return [part.astype(jnp.bfloat16) for part in (hi, mid, low)]


def attention_kernel(tokens, heads, head_size, tile, sources, *refs):
    valid_ref, docs_ref, q_ref, meta_ref, gain_ref = refs[:5]
    kv_refs = refs[5 : 5 + 2 * sources]
    mine_ref, other_ref = refs[5 + 2 * sources : 7 + 2 * sources]
    m_ref, l_ref, acc_ref = refs[7 + 2 * sources :]
    width = heads * head_size
    halves = tokens // width
    rows = tokens // head_size
    score_scale = head_size ** (-0.5) * LOG2E
    lane = lax.broadcasted_iota(jnp.int32, (1, width), 1)
    in_head = [(lane >= h * head_size) & (lane < (h + 1) * head_size) for h in range(heads)]

    def spread(parts):
        full = jnp.broadcast_to(parts[0], (tile, width))
        for h in range(1, heads):
            full = jnp.where(in_head[h], parts[h], full)
        return full

    def q_tile(step, carry):
        row0 = pl.multiple_of(step * tile, tile)
        q = q_ref[pl.ds(row0, tile), :]
        meta = meta_ref[pl.ds(row0, tile), :]
        q_doc = meta[:, heads : heads + 1]
        first_doc = docs_ref[row0].astype(jnp.float32)

        def visit(source):
            k_ref, v_ref = kv_refs[2 * source], kv_refs[2 * source + 1]
            k = k_ref[:tokens, :]
            v = v_ref[...]
            extra = k_ref[tokens:, :].astype(jnp.float32)
            gates = (extra[:rows] + extra[rows : 2 * rows] + extra[2 * rows : 3 * rows]) * LOG2E
            doc_rows = extra[3 * rows : 3 * rows + halves]
            k_doc = jnp.concatenate([doc_rows[j : j + 1] for j in range(halves)], axis=1)
            allowed = k_doc == q_doc
            if source == 0:
                q_pos = row0 + lax.broadcasted_iota(jnp.int32, (tile, tokens), 0)
                k_pos = lax.broadcasted_iota(jnp.int32, (tile, tokens), 1)
                allowed = allowed & (k_pos <= q_pos)
            total = jnp.zeros((tile, width), jnp.float32)
            rescales = []
            for h in range(heads):
                q_h = jnp.where(in_head[h], q, jnp.zeros((), q.dtype))
                s = lax.dot_general(
                    q_h, k, (((1,), (1,)), ((), ())), preferred_element_type=jnp.float32
                )
                gate_row = jnp.concatenate(
                    [gates[h * halves + j : h * halves + j + 1] for j in range(halves)], axis=1
                )
                s = s * score_scale + (meta[:, h : h + 1] * LOG2E - gate_row)
                s = jnp.where(allowed, s, NEG)
                block_max = jnp.max(s, axis=1, keepdims=True)
                if source == 0:
                    new_max = block_max
                else:
                    old_max = m_ref[h]
                    new_max = jnp.maximum(old_max, block_max)
                    rescale = jnp.exp2(old_max - new_max)
                    rescales.append(rescale)
                p = jnp.exp2(s - new_max)
                block_sum = jnp.sum(p, axis=1, keepdims=True)
                m_ref[h] = new_max
                l_ref[h] = block_sum if source == 0 else l_ref[h] * rescale + block_sum
                v_h = jnp.where(in_head[h], v, jnp.zeros((), v.dtype))
                total = total + jnp.dot(
                    p.astype(jnp.bfloat16), v_h, preferred_element_type=jnp.float32
                )
            if source == 0:
                acc_ref[...] = total
            else:
                acc_ref[...] = acc_ref[...] * spread(rescales) + total

        visit(0)
        for source in range(1, sources):
            last_doc = jnp.max(
                kv_refs[2 * source][tokens + 3 * rows : tokens + 3 * rows + halves, :].astype(
                    jnp.float32
                )
            )

            @pl.when((valid_ref[source] > 0) & (last_doc >= first_doc))
            def _():
                visit(source)

        attended = acc_ref[...] / spread([l_ref[h] for h in range(heads)])
        squares = attended * attended
        means = [
            jnp.sum(jnp.where(in_head[h], squares, 0.0), axis=1, keepdims=True) / head_size
            for h in range(heads)
        ]
        scale = spread([lax.rsqrt(mean + EPS) for mean in means])
        normed = (attended * scale * gain_ref[...]).astype(jnp.bfloat16)
        here = pl.ds(pl.multiple_of((step // 2) * tile, tile), tile)

        @pl.when(step % 2 == valid_ref[sources])
        def _():
            mine_ref[here, :] = normed

        @pl.when(step % 2 != valid_ref[sources])
        def _():
            other_ref[here, :] = normed

        return carry

    lax.fori_loop(0, tokens // tile, q_tile, 0)


def attend(queries, keys, values, cum_gate, documents, head_gain):
    tokens, width = queries.shape
    heads = cum_gate.shape[1]
    head_size = width // heads
    n_sp = lax.axis_size("sp")
    place = lax.axis_index("sp")
    tile = tokens // lax.axis_size("tp")

    gate_rows = [part.T.reshape(-1, width) for part in bf16_parts(cum_gate)]
    doc_rows = documents.astype(jnp.bfloat16).reshape(-1, width)
    used = sum(part.shape[0] for part in gate_rows) + doc_rows.shape[0]
    filler = jnp.zeros((-used % 16, width), jnp.bfloat16)
    keys_more = jnp.concatenate([keys, *gate_rows, doc_rows, filler], axis=0)
    meta = jnp.concatenate(
        [
            cum_gate,
            documents.astype(jnp.float32)[:, None],
            jnp.zeros((tokens, 8 - (heads + 1) % 8), jnp.float32),
        ],
        axis=1,
    )

    reach = n_sp // 4
    ahead = [(i, i + 2) for i in range(n_sp - 2)]
    even_up = [(i, i + 1) for i in range(0, n_sp, 2)]
    odd_down = [(i + 1, i) for i in range(0, n_sp, 2)]

    def chain(first):
        own, other = [first], []
        for step in range(reach + 1):
            pairs = even_up if step == 0 else odd_down if step == reach else even_up + odd_down
            if step > 0:
                own.append(lax.ppermute(own[-1], "sp", ahead))
            other.append(lax.ppermute(own[-1], "sp", pairs))
        return own, other

    key_own, key_other = chain(keys_more)
    value_own, value_other = chain(values)
    group, member = place // 2, place % 2
    blocks, valid = [], []
    for step in range(reach + 1):
        exists = group - step >= 0
        blocks += [key_own[step], value_own[step]]
        valid.append(exists)
        blocks += [key_other[step], value_other[step]]
        if step == 0:
            exists = exists & (member == 1)
        elif step == reach:
            exists = exists & (member == 0)
        valid.append(exists)
    sources = len(valid)
    valid = jnp.stack(valid + [lax.axis_index("tp") % 2 == 1]).astype(jnp.int32)

    def kernel(*refs):
        attention_kernel(tokens, heads, head_size, tile, sources, *refs)

    vmem = pl.BlockSpec(memory_space=pltpu.VMEM)
    smem = pl.BlockSpec(memory_space=pltpu.SMEM)
    return pl.pallas_call(
        kernel,
        out_shape=[jax.ShapeDtypeStruct((tokens // 2, width), jnp.bfloat16)] * 2,
        in_specs=[smem, smem] + [vmem] * (3 + len(blocks)),
        out_specs=[vmem, vmem],
        scratch_shapes=[
            pltpu.VMEM((heads, tile, 1), jnp.float32),
            pltpu.VMEM((heads, tile, 1), jnp.float32),
            pltpu.VMEM((tile, width), jnp.float32),
        ],
        compiler_params=pltpu.CompilerParams(vmem_limit_bytes=50 * 2**20),
        name="attention",
    )(valid, documents, queries, meta, head_gain[None, :], *blocks)


def swap(x, axis, bits):
    return lax.ppermute(x, axis, [(i, i ^ bits) for i in range(lax.axis_size(axis))])


def ways(n_sp):
    inner = n_sp // 4
    return [(step, bits) for step in range(4) for bits in range(inner)]


def both_blocks(way):
    return way in ((0, 0), (1, 0), (3, 0))


def expert_groups(n_sp):
    inner = n_sp // 4
    low, high = range(inner // 2), range(inner // 2, inner)
    return [
        [(0, bits) for bits in range(inner)],
        [(step, bits) for bits in low for step in (1, 3)],
        [(step, bits) for bits in high for step in (1, 3)],
        [(2, bits) for bits in range(inner)],
    ]


def move(x, way):
    step, bits = way
    n_sp = lax.axis_size("sp")
    inner = n_sp // 4
    return lax.ppermute(
        x,
        "sp",
        [(i, ((i // inner + step) % 4) * inner + ((i % inner) ^ bits)) for i in range(n_sp)],
    )


def expert_at(place, n_sp, way):
    inner = n_sp // 4
    return ((place // inner + way[0]) % 4) * inner + ((place % inner) ^ way[1])


def project_kernel(experts, capacity, n_tp, *refs):
    blocks = n_tp // 2
    place_ref = refs[0]
    pieces = refs[1 : 1 + n_tp]
    weight_ref = refs[1 + n_tp]
    resids = refs[2 + n_tp : 2 + n_tp + blocks]
    routes = refs[2 + n_tp + blocks : 2 + n_tp + 2 * blocks]
    gain_ref = refs[2 + n_tp + 2 * blocks]
    outs = refs[3 + n_tp + 2 * blocks : 3 + n_tp + 2 * blocks + experts]
    stream_ref, wide_ref, packed_ref, slot_ref, pick_ref = refs[3 + n_tp + 2 * blocks + experts :]
    rows, width = resids[0].shape
    part = pieces[0].shape[1]
    place, spot = place_ref[0], place_ref[1]
    across = spot // 2
    n_tile = 512

    inputs = [
        jnp.concatenate(
            [
                piece[pl.ds(pl.multiple_of((across ^ j) * rows, rows), rows), :]
                for j in range(blocks)
            ],
            axis=0,
        )
        for piece in pieces
    ]
    total = jnp.zeros((blocks * rows, 1), jnp.float32)
    for n in range(width // n_tile):
        cols = slice(n * n_tile, (n + 1) * n_tile)
        projected = jnp.zeros((blocks * rows, n_tile), jnp.float32)
        for k in range(n_tp):
            from_row = pl.multiple_of((spot ^ k) * part, part)
            projected = projected + jnp.dot(
                inputs[k],
                weight_ref[pl.ds(from_row, part), cols],
                preferred_element_type=jnp.float32,
            )
        resid = jnp.concatenate([resid_ref[:, cols] for resid_ref in resids], axis=0)
        stream = (resid.astype(jnp.float32) + projected).astype(jnp.bfloat16)
        stream_ref[:, cols] = stream[:rows]
        wide = stream.astype(jnp.float32)
        wide_ref[:, cols] = wide
        total = total + jnp.sum(wide * wide, axis=1, keepdims=True)
    scale = lax.rsqrt(total / width + EPS)

    before = (
        lax.broadcasted_iota(jnp.int32, (rows, rows), 0)
        < lax.broadcasted_iota(jnp.int32, (rows, rows), 1)
    ).astype(jnp.bfloat16)
    expert_ids = lax.broadcasted_iota(jnp.int32, (experts, rows), 0).astype(jnp.float32)
    for j in range(blocks):
        chosen = jnp.zeros((experts, rows), jnp.float32)
        for route in range(2):
            chosen = chosen + (routes[j][route : route + 1, :] == expert_ids).astype(jnp.float32)
        ranks = jnp.dot(chosen.astype(jnp.bfloat16), before, preferred_element_type=jnp.float32)
        slot_ref[j] = jnp.where(chosen > 0.0, ranks, -1.0)
    slot_ids = lax.broadcasted_iota(jnp.int32, (capacity, rows), 0).astype(jnp.float32)
    first, spans = 0, []
    for way in ways(experts):
        spans.append(first)
        expert = expert_at(place, experts, way)
        for j in range(blocks if both_blocks(way) else 1):
            row_of = slot_ref[j, pl.ds(expert, 1), :]
            for i in range(blocks):
                pick = (slot_ids == row_of) if i == j else jnp.zeros((capacity, rows), jnp.bool_)
                pick_ref[first : first + capacity, i * rows : (i + 1) * rows] = pick.astype(
                    jnp.float32
                ).astype(jnp.bfloat16)
            first += capacity
    spans.append(first)
    for n in range(width // n_tile):
        cols = slice(n * n_tile, (n + 1) * n_tile)
        packed_ref[...] = (wide_ref[:, cols] * scale * gain_ref[:, cols]).astype(jnp.bfloat16)
        picked = jnp.dot(
            pick_ref[...], packed_ref[...], preferred_element_type=jnp.float32
        ).astype(jnp.bfloat16)
        for k in range(experts):
            outs[k][:, cols] = picked[spans[k] : spans[k + 1]]


def expert_kernel(count, *refs):
    inputs = refs[:count]
    gate_ref, up_ref, down_hbm = refs[count : count + 3]
    mine_ref, other_ref, x_ref, hidden_ref, down_ref, sem = refs[count + 3 :]
    mine_rows = mine_ref.shape[0]
    step, steps = pl.program_id(0), hidden_ref.shape[0]
    fetch = pltpu.make_async_copy(down_hbm, down_ref, sem)

    @pl.when(step == 0)
    def _():
        fetch.start()
        row = 0
        for ref in inputs:
            x_ref[row : row + ref.shape[0], :] = ref[...]
            row += ref.shape[0]

    both = jnp.concatenate([gate_ref[...], up_ref[...]], axis=1)
    product = jnp.dot(x_ref[...], both, preferred_element_type=jnp.float32)
    half = product.shape[1] // 2
    gate, up = product[:, :half], product[:, half:]
    hidden_ref[step] = (gate * (1.0 / (1.0 + jnp.exp(-gate))) * up).astype(jnp.bfloat16)

    @pl.when(step == steps - 1)
    def _():
        fetch.wait()
        hidden = jnp.concatenate([hidden_ref[i] for i in range(steps)], axis=1)
        n_tile = 512
        for n in range(down_ref.shape[1] // n_tile):
            cols = slice(n * n_tile, (n + 1) * n_tile)
            out = jnp.dot(
                hidden, down_ref[:, cols], preferred_element_type=jnp.float32
            ).astype(jnp.bfloat16)
            mine_ref[:, cols] = out[:mine_rows]
            other_ref[:, cols] = out[mine_rows:]


def combine_kernel(experts, place_ref, stream_ref, routes_ref, weights_ref, *refs):
    outs = refs[:experts]
    mixed_ref, stack_ref = refs[experts:]
    rows, width = stream_ref.shape
    capacity = outs[0].shape[0]
    place, inner = place_ref[0], experts // 4
    for k in range(experts):
        stack_ref[k * capacity : (k + 1) * capacity, :] = outs[k][...]
    expert_ids = lax.broadcasted_iota(jnp.int32, (rows, experts), 1)
    named = [
        (routes_ref[:, route : route + 1] == expert_ids).astype(jnp.float32) for route in range(2)
    ]
    before = (
        lax.broadcasted_iota(jnp.int32, (rows, rows), 1)
        < lax.broadcasted_iota(jnp.int32, (rows, rows), 0)
    ).astype(jnp.bfloat16)
    ranks = jnp.dot(
        before, (named[0] + named[1]).astype(jnp.bfloat16), preferred_element_type=jnp.float32
    )
    slot_ids = lax.broadcasted_iota(jnp.int32, (rows, experts * capacity), 1)
    picks = []
    for route in range(2):
        rank = jnp.sum(named[route] * ranks, axis=1, keepdims=True).astype(jnp.int32)
        expert = routes_ref[:, route : route + 1]
        step = (expert // inner + 4 - place // inner) % 4
        target = (step * inner + ((expert % inner) ^ (place % inner))) * capacity + rank
        picks.append((slot_ids == target).astype(jnp.float32).astype(jnp.bfloat16))
    n_tile = 512
    for n in range(width // n_tile):
        cols = slice(n * n_tile, (n + 1) * n_tile)
        mixed = stream_ref[:, cols].astype(jnp.float32)
        for route in range(2):
            result = jnp.dot(picks[route], stack_ref[:, cols], preferred_element_type=jnp.float32)
            mixed = mixed + weights_ref[:, route : route + 1] * result
        mixed_ref[:, cols] = mixed.astype(jnp.bfloat16)


def on_device(
    queries,
    keys,
    values,
    cum_gate,
    documents,
    head_gain,
    out_weight,
    resid,
    norm_gain,
    routes,
    route_weights,
    w_gate,
    w_up,
    w_down,
):
    tokens = queries.shape[0]
    n_sp, n_tp = lax.axis_size("sp"), lax.axis_size("tp")
    place, spot = lax.axis_index("sp"), lax.axis_index("tp")
    blocks = n_tp // 2
    local_rows, model_width = resid.shape
    capacity = 2 * routes.shape[1] * tokens // (n_tp * n_sp)
    each = blocks * capacity
    vmem = pl.BlockSpec(memory_space=pltpu.VMEM)
    smem = pl.BlockSpec(memory_space=pltpu.SMEM)
    places = jnp.stack([place, spot]).astype(jnp.int32)

    route_rows = jnp.concatenate(
        [routes.T.astype(jnp.float32), jnp.zeros((8 - routes.shape[1], local_rows), jnp.float32)],
        axis=0,
    )
    resids = [resid] + [swap(resid, "tp", 2 * j) for j in range(1, blocks)]
    route_blocks = [route_rows] + [swap(route_rows, "tp", 2 * j) for j in range(1, blocks)]

    mine, other = attend(queries, keys, values, cum_gate, documents, head_gain)
    pieces = [mine] + [swap(other if k % 2 else mine, "tp", k) for k in range(1, n_tp)]

    counts = [each if both_blocks(way) else capacity for way in ways(n_sp)]

    def project(*refs):
        project_kernel(n_sp, capacity, n_tp, *refs)

    *outbound, stream = pl.pallas_call(
        project,
        out_shape=[jax.ShapeDtypeStruct((count, model_width), jnp.bfloat16) for count in counts]
        + [jax.ShapeDtypeStruct((local_rows, model_width), jnp.bfloat16)],
        in_specs=[smem] + [vmem] * (n_tp + 2 + 2 * blocks),
        out_specs=[vmem] * (n_sp + 1),
        scratch_shapes=[
            pltpu.VMEM((blocks * local_rows, model_width), jnp.float32),
            pltpu.VMEM((blocks * local_rows, 512), jnp.bfloat16),
            pltpu.VMEM((blocks, n_sp, local_rows), jnp.float32),
            pltpu.VMEM((sum(counts), blocks * local_rows), jnp.bfloat16),
        ],
        compiler_params=pltpu.CompilerParams(vmem_limit_bytes=40 * 2**20),
        name="project",
    )(places, *pieces, out_weight, *resids, *route_blocks, norm_gain[None, :])

    outbound = dict(zip(ways(n_sp), outbound))

    def dispatch(way):
        step, bits = way
        x = outbound[way]
        if way == (0, 0):
            return x
        if step == 0 or bits == 0:
            return move(x, way)
        x = move(x, (0, bits))
        if step == 2:
            x = move(x, (3, 0))
            return move(x, (3, 0))
        return move(x, (step, 0))

    groups = expert_groups(n_sp)
    members = len(groups[0])
    hidden_width = w_gate.shape[2]
    h_tile = 128
    rows = 2 * members * each
    arrived = {way: dispatch(way) for way in ways(n_sp)}
    returned = {}
    for group in groups:
        inputs = []
        for way in group:
            inputs.append(arrived[way])
            if not both_blocks(way):
                inputs += [swap(arrived[way], "tp", 2 * j) for j in range(1, blocks)]
        inputs += [swap(x, "tp", 1) for x in inputs]

        def expert(*refs):
            expert_kernel(len(inputs), *refs)

        part_mine, part_other = pl.pallas_call(
            expert,
            grid=(hidden_width // h_tile,),
            out_shape=[jax.ShapeDtypeStruct((members * each, model_width), jnp.bfloat16)] * 2,
            in_specs=[pl.BlockSpec(x.shape, lambda f: (0, 0)) for x in inputs]
            + [pl.BlockSpec((model_width, h_tile), lambda f: (0, f))] * 2
            + [pl.BlockSpec(memory_space=pl.ANY)],
            out_specs=[pl.BlockSpec((members * each, model_width), lambda f: (0, 0))] * 2,
            scratch_shapes=[
                pltpu.VMEM((rows, model_width), jnp.bfloat16),
                pltpu.VMEM((hidden_width // h_tile, rows, h_tile), jnp.bfloat16),
                pltpu.VMEM((hidden_width, model_width), jnp.bfloat16),
                pltpu.SemaphoreType.DMA,
            ],
            compiler_params=pltpu.CompilerParams(
                dimension_semantics=("arbitrary",), vmem_limit_bytes=40 * 2**20
            ),
            cost_estimate=pl.CostEstimate(
                flops=6 * rows * model_width * hidden_width,
                transcendentals=rows * hidden_width,
                bytes_accessed=6 * model_width * hidden_width + 4 * rows * model_width,
            ),
            name="expert",
        )(*inputs, w_gate[0], w_up[0], w_down[0])
        added = swap(part_other, "tp", 1)
        shape = (members, blocks, capacity, model_width)
        part_mine, added = part_mine.reshape(shape), added.reshape(shape)

        def summed(j):
            return part_mine[:, j].astype(jnp.float32) + added[:, j].astype(jnp.float32)

        result = summed(0)
        for j in range(1, blocks):
            sent = swap(summed(j).astype(jnp.bfloat16), "tp", 2 * j)
            result = result + sent.astype(jnp.float32)
        result = result.astype(jnp.bfloat16)
        for i, way in enumerate(group):
            back = (-way[0] % 4, way[1])
            returned[way] = result[i] if way == (0, 0) else move(result[i], back)

    def combine(*refs):
        combine_kernel(n_sp, *refs)

    return pl.pallas_call(
        combine,
        out_shape=jax.ShapeDtypeStruct((local_rows, model_width), jnp.bfloat16),
        in_specs=[smem] + [vmem] * (3 + n_sp),
        out_specs=vmem,
        scratch_shapes=[pltpu.VMEM((n_sp * capacity, model_width), jnp.bfloat16)],
        compiler_params=pltpu.CompilerParams(vmem_limit_bytes=24 * 2**20),
        name="combine",
    )(places, stream, routes, route_weights, *[returned[way] for way in ways(n_sp)])


def solution(mesh):
    in_specs = (
        P("sp", "tp"),
        P("sp", "tp"),
        P("sp", "tp"),
        P("sp", "tp"),
        P("sp"),
        P("tp"),
        P(),
        P(("sp", "tp"), None),
        P(),
        P(("sp", "tp"), None),
        P(("sp", "tp"), None),
        P("sp", None, "tp"),
        P("sp", None, "tp"),
        P("sp", "tp", None),
    )
    out_specs = P(("sp", "tp"), None)


    return jax.shard_map(on_device, mesh=mesh, in_specs=in_specs, out_specs=out_specs, check_vma=False)
```

```python
import jax
import jax.numpy as jnp
from jax import lax
from jax.experimental import pallas as pl
from jax.experimental.pallas import tpu as pltpu
from jax.sharding import PartitionSpec as P

EPS = 1e-06
LOG2E = 1.4426950408889634
NEG = -1e30


def bf16_parts(x):
    hi = lax.reduce_precision(x, 8, 7)
    rest = x - hi
    mid = lax.reduce_precision(rest, 8, 7)
    low = rest - mid
    return [part.astype(jnp.bfloat16) for part in (hi, mid, low)]


def attention_kernel(tokens, heads, head_size, tile, n_tp, sources, *refs):
    valid_ref, docs_ref, q_ref, meta_ref, gain_ref = refs[:5]
    kv_refs = refs[5 : 5 + 2 * sources]
    mine_ref, other_ref = refs[5 + 2 * sources : 7 + 2 * sources]
    m_ref, l_ref, acc_ref = refs[7 + 2 * sources :]
    width = heads * head_size
    halves = tokens // width
    rows = tokens // head_size
    score_scale = head_size ** (-0.5) * LOG2E
    lane = lax.broadcasted_iota(jnp.int32, (1, width), 1)
    in_head = [(lane >= h * head_size) & (lane < (h + 1) * head_size) for h in range(heads)]

    def spread(parts):
        full = jnp.broadcast_to(parts[0], (tile, width))
        for h in range(1, heads):
            full = jnp.where(in_head[h], parts[h], full)
        return full

    def q_tile(step, carry):
        row0 = pl.multiple_of(step * tile, tile)
        q = q_ref[pl.ds(row0, tile), :]
        meta = meta_ref[pl.ds(row0, tile), :]
        q_doc = meta[:, heads : heads + 1]
        first_doc = docs_ref[row0].astype(jnp.float32)

        def visit(source):
            k_ref, v_ref = kv_refs[2 * source], kv_refs[2 * source + 1]
            k = k_ref[:tokens, :]
            v = v_ref[...]
            extra = k_ref[tokens:, :].astype(jnp.float32)
            gates = (extra[:rows] + extra[rows : 2 * rows] + extra[2 * rows : 3 * rows]) * LOG2E
            doc_rows = extra[3 * rows : 3 * rows + halves]
            k_doc = jnp.concatenate([doc_rows[j : j + 1] for j in range(halves)], axis=1)
            allowed = k_doc == q_doc
            if source == 0:
                q_pos = row0 + lax.broadcasted_iota(jnp.int32, (tile, tokens), 0)
                k_pos = lax.broadcasted_iota(jnp.int32, (tile, tokens), 1)
                allowed = allowed & (k_pos <= q_pos)
            total = jnp.zeros((tile, width), jnp.float32)
            rescales = []
            for h in range(heads):
                q_h = jnp.where(in_head[h], q, jnp.zeros((), q.dtype))
                s = lax.dot_general(
                    q_h, k, (((1,), (1,)), ((), ())), preferred_element_type=jnp.float32
                )
                gate_row = jnp.concatenate(
                    [gates[h * halves + j : h * halves + j + 1] for j in range(halves)], axis=1
                )
                s = s * score_scale + (meta[:, h : h + 1] * LOG2E - gate_row)
                s = jnp.where(allowed, s, NEG)
                block_max = jnp.max(s, axis=1, keepdims=True)
                if source == 0:
                    new_max = block_max
                else:
                    old_max = m_ref[h]
                    new_max = jnp.maximum(old_max, block_max)
                    rescale = jnp.exp2(old_max - new_max)
                    rescales.append(rescale)
                p = jnp.exp2(s - new_max)
                block_sum = jnp.sum(p, axis=1, keepdims=True)
                m_ref[h] = new_max
                l_ref[h] = block_sum if source == 0 else l_ref[h] * rescale + block_sum
                v_h = jnp.where(in_head[h], v, jnp.zeros((), v.dtype))
                total = total + jnp.dot(
                    p.astype(jnp.bfloat16), v_h, preferred_element_type=jnp.float32
                )
            if source == 0:
                acc_ref[...] = total
            else:
                acc_ref[...] = acc_ref[...] * spread(rescales) + total

        visit(0)
        for source in range(1, sources):
            last_doc = jnp.max(
                kv_refs[2 * source][tokens + 3 * rows : tokens + 3 * rows + halves, :].astype(
                    jnp.float32
                )
            )

            @pl.when((valid_ref[source] > 0) & (last_doc >= first_doc))
            def _():
                visit(source)

        attended = acc_ref[...] / spread([l_ref[h] for h in range(heads)])
        squares = attended * attended
        means = [
            jnp.sum(jnp.where(in_head[h], squares, 0.0), axis=1, keepdims=True) / head_size
            for h in range(heads)
        ]
        scale = spread([lax.rsqrt(mean + EPS) for mean in means])
        normed = (attended * scale * gain_ref[...]).astype(jnp.bfloat16)
        piece = docs_ref.shape[0] // n_tp
        for part in range(tile // piece):
            index = step * (tile // piece) + part
            here = pl.ds(pl.multiple_of((index // 2) * piece, piece), piece)
            value = normed[part * piece : (part + 1) * piece]

            @pl.when(index % 2 == valid_ref[sources])
            def _():
                mine_ref[here, :] = value

            @pl.when(index % 2 != valid_ref[sources])
            def _():
                other_ref[here, :] = value

        return carry

    lax.fori_loop(0, tokens // tile, q_tile, 0)


def attend(queries, keys, values, cum_gate, documents, head_gain):
    tokens, width = queries.shape
    heads = cum_gate.shape[1]
    head_size = width // heads
    n_sp = lax.axis_size("sp")
    place = lax.axis_index("sp")
    tile = tokens // 2

    gate_rows = [part.T.reshape(-1, width) for part in bf16_parts(cum_gate)]
    doc_rows = documents.astype(jnp.bfloat16).reshape(-1, width)
    used = sum(part.shape[0] for part in gate_rows) + doc_rows.shape[0]
    filler = jnp.zeros((-used % 16, width), jnp.bfloat16)
    keys_more = jnp.concatenate([keys, *gate_rows, doc_rows, filler], axis=0)
    meta = jnp.concatenate(
        [
            cum_gate,
            documents.astype(jnp.float32)[:, None],
            jnp.zeros((tokens, 8 - (heads + 1) % 8), jnp.float32),
        ],
        axis=1,
    )

    reach = n_sp // 4
    ahead = [(i, i + 2) for i in range(n_sp - 2)]
    even_up = [(i, i + 1) for i in range(0, n_sp, 2)]
    odd_down = [(i + 1, i) for i in range(0, n_sp, 2)]

    def chain(first):
        own, other = [first], []
        for step in range(reach + 1):
            pairs = even_up if step == 0 else odd_down if step == reach else even_up + odd_down
            if step > 0:
                own.append(lax.ppermute(own[-1], "sp", ahead))
            other.append(lax.ppermute(own[-1], "sp", pairs))
        return own, other

    key_own, key_other = chain(keys_more)
    value_own, value_other = chain(values)
    group, member = place // 2, place % 2
    blocks, valid = [], []
    for step in range(reach + 1):
        exists = group - step >= 0
        blocks += [key_own[step], value_own[step]]
        valid.append(exists)
        blocks += [key_other[step], value_other[step]]
        if step == 0:
            exists = exists & (member == 1)
        elif step == reach:
            exists = exists & (member == 0)
        valid.append(exists)
    sources = len(valid)
    valid = jnp.stack(valid + [lax.axis_index("tp") % 2 == 1]).astype(jnp.int32)

    def kernel(*refs):
        attention_kernel(tokens, heads, head_size, tile, lax.axis_size("tp"), sources, *refs)

    vmem = pl.BlockSpec(memory_space=pltpu.VMEM)
    smem = pl.BlockSpec(memory_space=pltpu.SMEM)
    return pl.pallas_call(
        kernel,
        out_shape=[jax.ShapeDtypeStruct((tokens // 2, width), jnp.bfloat16)] * 2,
        in_specs=[smem, smem] + [vmem] * (3 + len(blocks)),
        out_specs=[vmem, vmem],
        scratch_shapes=[
            pltpu.VMEM((heads, tile, 1), jnp.float32),
            pltpu.VMEM((heads, tile, 1), jnp.float32),
            pltpu.VMEM((tile, width), jnp.float32),
        ],
        compiler_params=pltpu.CompilerParams(vmem_limit_bytes=50 * 2**20),
        name="attention",
    )(valid, documents, queries, meta, head_gain[None, :], *blocks)


def swap(x, axis, bits):
    return lax.ppermute(x, axis, [(i, i ^ bits) for i in range(lax.axis_size(axis))])


def ways(n_sp):
    inner = n_sp // 4
    return [(step, bits) for step in range(4) for bits in range(inner)]


def both_blocks(way):
    return way in ((0, 0), (1, 0), (3, 0))


def expert_groups(n_sp):
    inner = n_sp // 4
    low, high = range(inner // 2), range(inner // 2, inner)
    return [
        [(0, bits) for bits in range(inner)] + [(step, bits) for bits in low for step in (1, 3)],
        [(step, bits) for bits in high for step in (1, 3)],
        [(2, bits) for bits in range(inner)],
    ]


def move(x, way):
    step, bits = way
    n_sp = lax.axis_size("sp")
    inner = n_sp // 4
    return lax.ppermute(
        x,
        "sp",
        [(i, ((i // inner + step) % 4) * inner + ((i % inner) ^ bits)) for i in range(n_sp)],
    )


def expert_at(place, n_sp, way):
    inner = n_sp // 4
    return ((place // inner + way[0]) % 4) * inner + ((place % inner) ^ way[1])


def project_kernel(experts, capacity, n_tp, *refs):
    blocks = n_tp // 2
    place_ref = refs[0]
    pieces = refs[1 : 1 + n_tp]
    weight_ref = refs[1 + n_tp]
    resids = refs[2 + n_tp : 2 + n_tp + blocks]
    routes = refs[2 + n_tp + blocks : 2 + n_tp + 2 * blocks]
    gain_ref = refs[2 + n_tp + 2 * blocks]
    outs = refs[3 + n_tp + 2 * blocks : 3 + n_tp + 2 * blocks + experts]
    stream_ref, wide_ref, packed_ref, slot_ref, pick_ref = refs[3 + n_tp + 2 * blocks + experts :]
    rows, width = resids[0].shape
    part = pieces[0].shape[1]
    place, spot = place_ref[0], place_ref[1]
    across = spot // 2
    n_tile = 512

    inputs = [
        jnp.concatenate(
            [
                piece[pl.ds(pl.multiple_of((across ^ j) * rows, rows), rows), :]
                for j in range(blocks)
            ],
            axis=0,
        )
        for piece in pieces
    ]
    total = jnp.zeros((blocks * rows, 1), jnp.float32)
    for n in range(width // n_tile):
        cols = slice(n * n_tile, (n + 1) * n_tile)
        projected = jnp.zeros((blocks * rows, n_tile), jnp.float32)
        for k in range(n_tp):
            from_row = pl.multiple_of((spot ^ k) * part, part)
            projected = projected + jnp.dot(
                inputs[k],
                weight_ref[pl.ds(from_row, part), cols],
                preferred_element_type=jnp.float32,
            )
        resid = jnp.concatenate([resid_ref[:, cols] for resid_ref in resids], axis=0)
        stream = (resid.astype(jnp.float32) + projected).astype(jnp.bfloat16)
        stream_ref[:, cols] = stream[:rows]
        wide = stream.astype(jnp.float32)
        wide_ref[:, cols] = wide
        total = total + jnp.sum(wide * wide, axis=1, keepdims=True)
    scale = lax.rsqrt(total / width + EPS)

    before = (
        lax.broadcasted_iota(jnp.int32, (rows, rows), 0)
        < lax.broadcasted_iota(jnp.int32, (rows, rows), 1)
    ).astype(jnp.bfloat16)
    expert_ids = lax.broadcasted_iota(jnp.int32, (experts, rows), 0).astype(jnp.float32)
    for j in range(blocks):
        chosen = jnp.zeros((experts, rows), jnp.float32)
        for route in range(2):
            chosen = chosen + (routes[j][route : route + 1, :] == expert_ids).astype(jnp.float32)
        ranks = jnp.dot(chosen.astype(jnp.bfloat16), before, preferred_element_type=jnp.float32)
        slot_ref[j] = jnp.where(chosen > 0.0, ranks, -1.0)
    slot_ids = lax.broadcasted_iota(jnp.int32, (capacity, rows), 0).astype(jnp.float32)
    first, spans = 0, []
    for way in ways(experts):
        spans.append(first)
        expert = expert_at(place, experts, way)
        for j in range(blocks if both_blocks(way) else 1):
            row_of = slot_ref[j, pl.ds(expert, 1), :]
            for i in range(blocks):
                pick = (slot_ids == row_of) if i == j else jnp.zeros((capacity, rows), jnp.bool_)
                pick_ref[first : first + capacity, i * rows : (i + 1) * rows] = pick.astype(
                    jnp.float32
                ).astype(jnp.bfloat16)
            first += capacity
    spans.append(first)
    for n in range(width // n_tile):
        cols = slice(n * n_tile, (n + 1) * n_tile)
        packed_ref[...] = (wide_ref[:, cols] * scale * gain_ref[:, cols]).astype(jnp.bfloat16)
        picked = jnp.dot(
            pick_ref[...], packed_ref[...], preferred_element_type=jnp.float32
        ).astype(jnp.bfloat16)
        for k in range(experts):
            outs[k][:, cols] = picked[spans[k] : spans[k + 1]]


def expert_kernel(count, moves, *refs):
    inputs = refs[:count]
    gate_ref, up_ref, down_hbm = refs[count : count + 3]
    mine_ref, other_ref, x_ref, hidden_ref, down_ref, sem = refs[count + 3 :]
    mine_rows = mine_ref.shape[0]
    step, steps = pl.program_id(0), hidden_ref.shape[0]
    fetch = pltpu.make_async_copy(down_hbm, down_ref, sem)

    @pl.when(step == 0)
    def _():
        fetch.start()
        row = 0
        for ref in inputs:
            x_ref[row : row + ref.shape[0], :] = ref[...]
            row += ref.shape[0]

    both = jnp.concatenate([gate_ref[...], up_ref[...]], axis=1)
    product = jnp.dot(x_ref[...], both, preferred_element_type=jnp.float32)
    half = product.shape[1] // 2
    gate, up = product[:, :half], product[:, half:]
    hidden_ref[step] = (gate * (1.0 / (1.0 + jnp.exp(-gate))) * up).astype(jnp.bfloat16)

    @pl.when(step == steps - 1)
    def _():
        fetch.wait()
        hidden = jnp.concatenate([hidden_ref[i] for i in range(steps)], axis=1)
        n_tile = 512
        for n in range(down_ref.shape[1] // n_tile):
            cols = slice(n * n_tile, (n + 1) * n_tile)
            out = jnp.dot(
                hidden, down_ref[:, cols], preferred_element_type=jnp.float32
            ).astype(jnp.bfloat16)
            for source, target, span in moves:
                mine_ref[target : target + span, cols] = out[source : source + span]
                source += mine_rows
                other_ref[target : target + span, cols] = out[source : source + span]


def combine_kernel(experts, place_ref, stream_ref, routes_ref, weights_ref, *refs):
    outs = refs[:experts]
    mixed_ref, stack_ref = refs[experts:]
    rows, width = stream_ref.shape
    capacity = outs[0].shape[0]
    place, inner = place_ref[0], experts // 4
    for k in range(experts):
        stack_ref[k * capacity : (k + 1) * capacity, :] = outs[k][...]
    expert_ids = lax.broadcasted_iota(jnp.int32, (rows, experts), 1)
    named = [
        (routes_ref[:, route : route + 1] == expert_ids).astype(jnp.float32) for route in range(2)
    ]
    before = (
        lax.broadcasted_iota(jnp.int32, (rows, rows), 1)
        < lax.broadcasted_iota(jnp.int32, (rows, rows), 0)
    ).astype(jnp.bfloat16)
    ranks = jnp.dot(
        before, (named[0] + named[1]).astype(jnp.bfloat16), preferred_element_type=jnp.float32
    )
    slot_ids = lax.broadcasted_iota(jnp.int32, (rows, experts * capacity), 1)
    picks = []
    for route in range(2):
        rank = jnp.sum(named[route] * ranks, axis=1, keepdims=True).astype(jnp.int32)
        expert = routes_ref[:, route : route + 1]
        step = (expert // inner + 4 - place // inner) % 4
        target = (step * inner + ((expert % inner) ^ (place % inner))) * capacity + rank
        picks.append((slot_ids == target).astype(jnp.float32).astype(jnp.bfloat16))
    n_tile = 512
    for n in range(width // n_tile):
        cols = slice(n * n_tile, (n + 1) * n_tile)
        mixed = stream_ref[:, cols].astype(jnp.float32)
        for route in range(2):
            result = jnp.dot(picks[route], stack_ref[:, cols], preferred_element_type=jnp.float32)
            mixed = mixed + weights_ref[:, route : route + 1] * result
        mixed_ref[:, cols] = mixed.astype(jnp.bfloat16)


def on_device(
    queries,
    keys,
    values,
    cum_gate,
    documents,
    head_gain,
    out_weight,
    resid,
    norm_gain,
    routes,
    route_weights,
    w_gate,
    w_up,
    w_down,
):
    tokens = queries.shape[0]
    n_sp, n_tp = lax.axis_size("sp"), lax.axis_size("tp")
    place, spot = lax.axis_index("sp"), lax.axis_index("tp")
    blocks = n_tp // 2
    local_rows, model_width = resid.shape
    capacity = 2 * routes.shape[1] * tokens // (n_tp * n_sp)
    each = blocks * capacity
    vmem = pl.BlockSpec(memory_space=pltpu.VMEM)
    smem = pl.BlockSpec(memory_space=pltpu.SMEM)
    places = jnp.stack([place, spot]).astype(jnp.int32)

    route_rows = jnp.concatenate(
        [routes.T.astype(jnp.float32), jnp.zeros((8 - routes.shape[1], local_rows), jnp.float32)],
        axis=0,
    )
    resids = [resid] + [swap(resid, "tp", 2 * j) for j in range(1, blocks)]
    route_blocks = [route_rows] + [swap(route_rows, "tp", 2 * j) for j in range(1, blocks)]

    mine, other = attend(queries, keys, values, cum_gate, documents, head_gain)
    pieces = [mine] + [swap(other if k % 2 else mine, "tp", k) for k in range(1, n_tp)]

    counts = [each if both_blocks(way) else capacity for way in ways(n_sp)]

    def project(*refs):
        project_kernel(n_sp, capacity, n_tp, *refs)

    *outbound, stream = pl.pallas_call(
        project,
        out_shape=[jax.ShapeDtypeStruct((count, model_width), jnp.bfloat16) for count in counts]
        + [jax.ShapeDtypeStruct((local_rows, model_width), jnp.bfloat16)],
        in_specs=[smem] + [vmem] * (n_tp + 2 + 2 * blocks),
        out_specs=[vmem] * (n_sp + 1),
        scratch_shapes=[
            pltpu.VMEM((blocks * local_rows, model_width), jnp.float32),
            pltpu.VMEM((blocks * local_rows, 512), jnp.bfloat16),
            pltpu.VMEM((blocks, n_sp, local_rows), jnp.float32),
            pltpu.VMEM((sum(counts), blocks * local_rows), jnp.bfloat16),
        ],
        compiler_params=pltpu.CompilerParams(vmem_limit_bytes=40 * 2**20),
        name="project",
    )(places, *pieces, out_weight, *resids, *route_blocks, norm_gain[None, :])

    outbound = dict(zip(ways(n_sp), outbound))

    def dispatch(way):
        step, bits = way
        x = outbound[way]
        if way == (0, 0):
            return x
        if step == 0 or bits == 0:
            return move(x, way)
        x = move(x, (0, bits))
        if step == 2:
            x = move(x, (3, 0))
            return move(x, (3, 0))
        return move(x, (step, 0))

    groups = expert_groups(n_sp)
    hidden_width = w_gate.shape[2]
    h_tile = 128
    arrived = {way: dispatch(way) for way in ways(n_sp)}
    returned = {}
    for group in groups:
        members = len(group)
        rows = 2 * members * each
        single = [way for way in group if not both_blocks(way)]
        both = [way for way in group if both_blocks(way)]
        inputs = [arrived[way] for way in both]
        moves = [
            (i * each + j * capacity, (j * members + i) * capacity, capacity)
            for i in range(len(both))
            for j in range(blocks)
        ]
        cut, count = len(both) * each, len(single) * capacity
        moves += [
            (cut + j * count, (j * members + len(both)) * capacity, count) for j in range(blocks)
        ]
        if len(single) > 1:
            joined = jnp.concatenate([arrived[way] for way in single], axis=0)
        else:
            joined = arrived[single[0]]
        crossed = [swap(joined, "tp", 2 * j) for j in range(1, blocks)]
        inputs += [joined, *crossed]
        inputs += [swap(x, "tp", 1) for x in inputs]

        def expert(*refs):
            expert_kernel(len(inputs), moves, *refs)

        part_mine, part_other = pl.pallas_call(
            expert,
            grid=(hidden_width // h_tile,),
            out_shape=[jax.ShapeDtypeStruct((members * each, model_width), jnp.bfloat16)] * 2,
            in_specs=[pl.BlockSpec(x.shape, lambda f: (0, 0)) for x in inputs]
            + [pl.BlockSpec((model_width, h_tile), lambda f: (0, f))] * 2
            + [pl.BlockSpec(memory_space=pl.ANY)],
            out_specs=[pl.BlockSpec((members * each, model_width), lambda f: (0, 0))] * 2,
            scratch_shapes=[
                pltpu.VMEM((rows, model_width), jnp.bfloat16),
                pltpu.VMEM((hidden_width // h_tile, rows, h_tile), jnp.bfloat16),
                pltpu.VMEM((hidden_width, model_width), jnp.bfloat16),
                pltpu.SemaphoreType.DMA,
            ],
            compiler_params=pltpu.CompilerParams(
                dimension_semantics=("arbitrary",), vmem_limit_bytes=40 * 2**20
            ),
            cost_estimate=pl.CostEstimate(
                flops=6 * rows * model_width * hidden_width,
                transcendentals=rows * hidden_width,
                bytes_accessed=6 * model_width * hidden_width + 4 * rows * model_width,
            ),
            name="expert",
        )(*inputs, w_gate[0], w_up[0], w_down[0])
        added = swap(part_other, "tp", 1)
        span = members * capacity

        def summed(j):
            here = slice(j * span, (j + 1) * span)
            return part_mine[here].astype(jnp.float32) + added[here].astype(jnp.float32)

        result = summed(0)
        for j in range(1, blocks):
            sent = swap(summed(j).astype(jnp.bfloat16), "tp", 2 * j)
            result = result + sent.astype(jnp.float32)
        result = result.astype(jnp.bfloat16).reshape(members, capacity, model_width)
        for i, way in enumerate(both + single):
            back = (-way[0] % 4, way[1])
            returned[way] = result[i] if way == (0, 0) else move(result[i], back)

    def combine(*refs):
        combine_kernel(n_sp, *refs)

    return pl.pallas_call(
        combine,
        out_shape=jax.ShapeDtypeStruct((local_rows, model_width), jnp.bfloat16),
        in_specs=[smem] + [vmem] * (3 + n_sp),
        out_specs=vmem,
        scratch_shapes=[pltpu.VMEM((n_sp * capacity, model_width), jnp.bfloat16)],
        compiler_params=pltpu.CompilerParams(vmem_limit_bytes=24 * 2**20),
        name="combine",
    )(places, stream, routes, route_weights, *[returned[way] for way in ways(n_sp)])


def solution(mesh):
    in_specs = (
        P("sp", "tp"),
        P("sp", "tp"),
        P("sp", "tp"),
        P("sp", "tp"),
        P("sp"),
        P("tp"),
        P(),
        P(("sp", "tp"), None),
        P(),
        P(("sp", "tp"), None),
        P(("sp", "tp"), None),
        P("sp", None, "tp"),
        P("sp", None, "tp"),
        P("sp", "tp", None),
    )
    out_specs = P(("sp", "tp"), None)


    return jax.shard_map(on_device, mesh=mesh, in_specs=in_specs, out_specs=out_specs, check_vma=False)
```

```python
import jax
import jax.numpy as jnp
from jax import lax
from jax.experimental import pallas as pl
from jax.experimental.pallas import tpu as pltpu
from jax.sharding import PartitionSpec as P

EPS = 1e-06
LOG2E = 1.4426950408889634
NEG = -1e30


def bf16_parts(x):
    hi = lax.reduce_precision(x, 8, 7)
    rest = x - hi
    mid = lax.reduce_precision(rest, 8, 7)
    low = rest - mid
    return [part.astype(jnp.bfloat16) for part in (hi, mid, low)]


def attention_kernel(tokens, heads, head_size, tile, sources, *refs):
    valid_ref, docs_ref, q_ref, meta_ref, gain_ref = refs[:5]
    kv_refs = refs[5 : 5 + 2 * sources]
    out_ref, m_ref, l_ref, acc_ref = refs[5 + 2 * sources :]
    width = heads * head_size
    halves = tokens // width
    rows = tokens // head_size
    score_scale = head_size ** (-0.5) * LOG2E
    lane = lax.broadcasted_iota(jnp.int32, (1, width), 1)
    in_head = [(lane >= h * head_size) & (lane < (h + 1) * head_size) for h in range(heads)]

    def spread(parts):
        full = jnp.broadcast_to(parts[0], (tile, width))
        for h in range(1, heads):
            full = jnp.where(in_head[h], parts[h], full)
        return full

    def q_tile(step, carry):
        row0 = pl.multiple_of(step * tile, tile)
        q = q_ref[pl.ds(row0, tile), :]
        meta = meta_ref[pl.ds(row0, tile), :]
        q_doc = meta[:, heads : heads + 1]
        first_doc = docs_ref[row0].astype(jnp.float32)

        def visit(source):
            k_ref, v_ref = kv_refs[2 * source], kv_refs[2 * source + 1]
            k = k_ref[:tokens, :]
            v = v_ref[...]
            extra = k_ref[tokens:, :].astype(jnp.float32)
            gates = (extra[:rows] + extra[rows : 2 * rows] + extra[2 * rows : 3 * rows]) * LOG2E
            doc_rows = extra[3 * rows : 3 * rows + halves]
            k_doc = jnp.concatenate([doc_rows[j : j + 1] for j in range(halves)], axis=1)
            allowed = k_doc == q_doc
            if source == 0:
                q_pos = row0 + lax.broadcasted_iota(jnp.int32, (tile, tokens), 0)
                k_pos = lax.broadcasted_iota(jnp.int32, (tile, tokens), 1)
                allowed = allowed & (k_pos <= q_pos)
            total = jnp.zeros((tile, width), jnp.float32)
            rescales = []
            for h in range(heads):
                q_h = jnp.where(in_head[h], q, jnp.zeros((), q.dtype))
                s = lax.dot_general(
                    q_h, k, (((1,), (1,)), ((), ())), preferred_element_type=jnp.float32
                )
                gate_row = jnp.concatenate(
                    [gates[h * halves + j : h * halves + j + 1] for j in range(halves)], axis=1
                )
                s = s * score_scale + (meta[:, h : h + 1] * LOG2E - gate_row)
                s = jnp.where(allowed, s, NEG)
                block_max = jnp.max(s, axis=1, keepdims=True)
                if source == 0:
                    new_max = block_max
                else:
                    old_max = m_ref[h]
                    new_max = jnp.maximum(old_max, block_max)
                    rescale = jnp.exp2(old_max - new_max)
                    rescales.append(rescale)
                p = jnp.exp2(s - new_max)
                block_sum = jnp.sum(p, axis=1, keepdims=True)
                m_ref[h] = new_max
                l_ref[h] = block_sum if source == 0 else l_ref[h] * rescale + block_sum
                v_h = jnp.where(in_head[h], v, jnp.zeros((), v.dtype))
                total = total + jnp.dot(
                    p.astype(jnp.bfloat16), v_h, preferred_element_type=jnp.float32
                )
            if source == 0:
                acc_ref[...] = total
            else:
                acc_ref[...] = acc_ref[...] * spread(rescales) + total

        visit(0)
        for source in range(1, sources):
            last_doc = jnp.max(
                kv_refs[2 * source][tokens + 3 * rows : tokens + 3 * rows + halves, :].astype(
                    jnp.float32
                )
            )

            @pl.when((valid_ref[source] > 0) & (last_doc >= first_doc))
            def _():
                visit(source)

        attended = acc_ref[...] / spread([l_ref[h] for h in range(heads)])
        squares = attended * attended
        means = [
            jnp.sum(jnp.where(in_head[h], squares, 0.0), axis=1, keepdims=True) / head_size
            for h in range(heads)
        ]
        scale = spread([lax.rsqrt(mean + EPS) for mean in means])
        out_ref[pl.ds(row0, tile), :] = (attended * scale * gain_ref[...]).astype(jnp.bfloat16)
        return carry

    lax.fori_loop(0, tokens // tile, q_tile, 0)


def attend(queries, keys, values, cum_gate, documents, head_gain):
    tokens, width = queries.shape
    heads = cum_gate.shape[1]
    head_size = width // heads
    n_sp = lax.axis_size("sp")
    place = lax.axis_index("sp")
    tile = tokens // 2

    gate_rows = [part.T.reshape(-1, width) for part in bf16_parts(cum_gate)]
    doc_rows = documents.astype(jnp.bfloat16).reshape(-1, width)
    used = sum(part.shape[0] for part in gate_rows) + doc_rows.shape[0]
    filler = jnp.zeros((-used % 16, width), jnp.bfloat16)
    keys_more = jnp.concatenate([keys, *gate_rows, doc_rows, filler], axis=0)
    meta = jnp.concatenate(
        [
            cum_gate,
            documents.astype(jnp.float32)[:, None],
            jnp.zeros((tokens, 8 - (heads + 1) % 8), jnp.float32),
        ],
        axis=1,
    )

    reach = n_sp // 4
    ahead = [(i, i + 2) for i in range(n_sp - 2)]
    even_up = [(i, i + 1) for i in range(0, n_sp, 2)]
    odd_down = [(i + 1, i) for i in range(0, n_sp, 2)]

    def chain(first):
        own, other = [first], []
        for step in range(reach + 1):
            pairs = even_up if step == 0 else odd_down if step == reach else even_up + odd_down
            if step > 0:
                own.append(lax.ppermute(own[-1], "sp", ahead))
            other.append(lax.ppermute(own[-1], "sp", pairs))
        return own, other

    key_own, key_other = chain(keys_more)
    value_own, value_other = chain(values)
    group, member = place // 2, place % 2
    blocks, valid = [], []
    for step in range(reach + 1):
        exists = group - step >= 0
        blocks += [key_own[step], value_own[step]]
        valid.append(exists)
        blocks += [key_other[step], value_other[step]]
        if step == 0:
            exists = exists & (member == 1)
        elif step == reach:
            exists = exists & (member == 0)
        valid.append(exists)
    sources = len(valid)
    valid = jnp.stack(valid).astype(jnp.int32)

    def kernel(*refs):
        attention_kernel(tokens, heads, head_size, tile, sources, *refs)

    vmem = pl.BlockSpec(memory_space=pltpu.VMEM)
    smem = pl.BlockSpec(memory_space=pltpu.SMEM)
    return pl.pallas_call(
        kernel,
        out_shape=jax.ShapeDtypeStruct((tokens, width), jnp.bfloat16),
        in_specs=[smem, smem] + [vmem] * (3 + len(blocks)),
        out_specs=vmem,
        scratch_shapes=[
            pltpu.VMEM((heads, tile, 1), jnp.float32),
            pltpu.VMEM((heads, tile, 1), jnp.float32),
            pltpu.VMEM((tile, width), jnp.float32),
        ],
        compiler_params=pltpu.CompilerParams(vmem_limit_bytes=50 * 2**20),
        name="attention",
    )(valid, documents, queries, meta, head_gain[None, :], *blocks)


def swap(x, axis, bits):
    return lax.ppermute(x, axis, [(i, i ^ bits) for i in range(lax.axis_size(axis))])


CHUNKS = 2


def project_kernel(experts, capacity, x_ref, weight_ref, resid_ref, routes_ref, gain_ref, *refs):
    outs = refs[:CHUNKS]
    stream_ref, wide_ref, pick_ref = refs[CHUNKS:]
    rows, width = resid_ref.shape
    n_tile = 512
    total = jnp.zeros((rows, 1), jnp.float32)
    for n in range(width // n_tile):
        cols = slice(n * n_tile, (n + 1) * n_tile)
        projected = jnp.dot(x_ref[...], weight_ref[:, cols], preferred_element_type=jnp.float32)
        stream = (resid_ref[:, cols].astype(jnp.float32) + projected).astype(jnp.bfloat16)
        stream_ref[:, cols] = stream
        wide = stream.astype(jnp.float32)
        wide_ref[:, cols] = wide
        total = total + jnp.sum(wide * wide, axis=1, keepdims=True)
    scale = lax.rsqrt(total / width + EPS)

    before = (
        lax.broadcasted_iota(jnp.int32, (rows, rows), 0)
        < lax.broadcasted_iota(jnp.int32, (rows, rows), 1)
    ).astype(jnp.bfloat16)
    expert_ids = lax.broadcasted_iota(jnp.int32, (experts, rows), 0).astype(jnp.float32)
    chosen = jnp.zeros((experts, rows), jnp.float32)
    for route in range(2):
        chosen = chosen + (routes_ref[route : route + 1, :] == expert_ids).astype(jnp.float32)
    ranks = jnp.dot(chosen.astype(jnp.bfloat16), before, preferred_element_type=jnp.float32)
    slots = jnp.where(chosen > 0.0, ranks, -1.0)
    span = capacity // CHUNKS
    for c in range(CHUNKS):
        slot_ids = lax.broadcasted_iota(jnp.int32, (span, rows), 0) + c * span
        for e in range(experts):
            pick = (slot_ids.astype(jnp.float32) == slots[e : e + 1, :]).astype(jnp.float32)
            first = (c * experts + e) * span
            pick_ref[first : first + span, :] = pick
    each = experts * span
    picks = pick_ref[...].astype(jnp.bfloat16)
    for n in range(width // n_tile):
        cols = slice(n * n_tile, (n + 1) * n_tile)
        normed = (wide_ref[:, cols] * scale * gain_ref[:, cols]).astype(jnp.bfloat16)
        picked = jnp.dot(picks, normed, preferred_element_type=jnp.float32).astype(jnp.bfloat16)
        for c in range(CHUNKS):
            outs[c][:, cols] = picked[c * each : (c + 1) * each]


def expert_kernel(count, *refs):
    inputs = refs[:count]
    gate_ref, up_ref, down_hbm = refs[count : count + 3]
    mine_ref, other_ref, x_ref, hidden_ref, down_ref, sem = refs[count + 3 :]
    mine_rows = mine_ref.shape[0]
    step, steps = pl.program_id(0), hidden_ref.shape[0]
    fetch = pltpu.make_async_copy(down_hbm, down_ref, sem)

    @pl.when(step == 0)
    def _():
        fetch.start()
        row = 0
        for ref in inputs:
            x_ref[row : row + ref.shape[0], :] = ref[...]
            row += ref.shape[0]

    both = jnp.concatenate([gate_ref[...], up_ref[...]], axis=1)
    product = jnp.dot(x_ref[...], both, preferred_element_type=jnp.float32)
    half = product.shape[1] // 2
    gate, up = product[:, :half], product[:, half:]
    hidden_ref[step] = (gate * (1.0 / (1.0 + jnp.exp(-gate))) * up).astype(jnp.bfloat16)

    @pl.when(step == steps - 1)
    def _():
        fetch.wait()
        hidden = jnp.concatenate([hidden_ref[i] for i in range(steps)], axis=1)
        n_tile = 512
        for n in range(down_ref.shape[1] // n_tile):
            cols = slice(n * n_tile, (n + 1) * n_tile)
            out = jnp.dot(
                hidden, down_ref[:, cols], preferred_element_type=jnp.float32
            ).astype(jnp.bfloat16)
            mine_ref[:, cols] = out[:mine_rows]
            other_ref[:, cols] = out[mine_rows:]


def combine_kernel(experts, stream_ref, routes_ref, weights_ref, *refs):
    outs = refs[:CHUNKS]
    mixed_ref, stack_ref = refs[CHUNKS:]
    rows, width = stream_ref.shape
    each = outs[0].shape[0]
    span = each // experts
    for c in range(CHUNKS):
        stack_ref[c * each : (c + 1) * each, :] = outs[c][...]
    expert_ids = lax.broadcasted_iota(jnp.int32, (rows, experts), 1)
    named = [
        (routes_ref[:, route : route + 1] == expert_ids).astype(jnp.float32) for route in range(2)
    ]
    before = (
        lax.broadcasted_iota(jnp.int32, (rows, rows), 1)
        < lax.broadcasted_iota(jnp.int32, (rows, rows), 0)
    ).astype(jnp.bfloat16)
    ranks = jnp.dot(
        before, (named[0] + named[1]).astype(jnp.bfloat16), preferred_element_type=jnp.float32
    )
    slot_ids = lax.broadcasted_iota(jnp.int32, (rows, CHUNKS * each), 1)
    picks = []
    for route in range(2):
        rank = jnp.sum(named[route] * ranks, axis=1, keepdims=True).astype(jnp.int32)
        chunk = rank // span
        target = chunk * each + routes_ref[:, route : route + 1] * span + (rank - chunk * span)
        picks.append((slot_ids == target).astype(jnp.float32).astype(jnp.bfloat16))
    n_tile = 512
    for n in range(width // n_tile):
        cols = slice(n * n_tile, (n + 1) * n_tile)
        mixed = stream_ref[:, cols].astype(jnp.float32)
        for route in range(2):
            result = jnp.dot(picks[route], stack_ref[:, cols], preferred_element_type=jnp.float32)
            mixed = mixed + weights_ref[:, route : route + 1] * result
        mixed_ref[:, cols] = mixed.astype(jnp.bfloat16)


def on_device(
    queries,
    keys,
    values,
    cum_gate,
    documents,
    head_gain,
    out_weight,
    resid,
    norm_gain,
    routes,
    route_weights,
    w_gate,
    w_up,
    w_down,
):
    tokens = queries.shape[0]
    n_sp, n_tp = lax.axis_size("sp"), lax.axis_size("tp")
    blocks = n_tp // 2
    local_rows, model_width = resid.shape
    capacity = 2 * routes.shape[1] * tokens // (n_tp * n_sp)
    span = capacity // CHUNKS
    vmem = pl.BlockSpec(memory_space=pltpu.VMEM)
    route_rows = routes.T.astype(jnp.float32)

    head_normed = attend(queries, keys, values, cum_gate, documents, head_gain)
    regrouped = lax.all_to_all(head_normed, "tp", split_axis=0, concat_axis=1, tiled=True)

    def project(*refs):
        project_kernel(n_sp, capacity, *refs)

    *outbound, stream = pl.pallas_call(
        project,
        out_shape=[jax.ShapeDtypeStruct((n_sp * span, model_width), jnp.bfloat16)] * CHUNKS
        + [jax.ShapeDtypeStruct((local_rows, model_width), jnp.bfloat16)],
        in_specs=[vmem] * 5,
        out_specs=[vmem] * (CHUNKS + 1),
        scratch_shapes=[
            pltpu.VMEM((local_rows, model_width), jnp.float32),
            pltpu.VMEM((n_sp * capacity, local_rows), jnp.float32),
        ],
        compiler_params=pltpu.CompilerParams(vmem_limit_bytes=40 * 2**20),
        name="project",
    )(regrouped, out_weight, resid, route_rows, norm_gain[None, :])

    hidden_width = w_gate.shape[2]
    h_tile = 128
    each = n_sp * span
    rows = n_tp * each
    arrived, crossed = [], []
    for c in range(CHUNKS):
        arrived.append(lax.all_to_all(outbound[c], "sp", 0, 0, tiled=True))
        crossed.append([swap(arrived[c], "tp", 2 * j) for j in range(1, blocks)])
    returned = []
    for c in range(CHUNKS):
        inputs = [arrived[c], *crossed[c]]
        inputs += [swap(x, "tp", 1) for x in inputs]

        def expert(*refs):
            expert_kernel(n_tp, *refs)

        part_mine, part_other = pl.pallas_call(
            expert,
            grid=(hidden_width // h_tile,),
            out_shape=[jax.ShapeDtypeStruct((rows // 2, model_width), jnp.bfloat16)] * 2,
            in_specs=[pl.BlockSpec(x.shape, lambda f: (0, 0)) for x in inputs]
            + [pl.BlockSpec((model_width, h_tile), lambda f: (0, f))] * 2
            + [pl.BlockSpec(memory_space=pl.ANY)],
            out_specs=[pl.BlockSpec((rows // 2, model_width), lambda f: (0, 0))] * 2,
            scratch_shapes=[
                pltpu.VMEM((rows, model_width), jnp.bfloat16),
                pltpu.VMEM((hidden_width // h_tile, rows, h_tile), jnp.bfloat16),
                pltpu.VMEM((hidden_width, model_width), jnp.bfloat16),
                pltpu.SemaphoreType.DMA,
            ],
            compiler_params=pltpu.CompilerParams(
                dimension_semantics=("arbitrary",), vmem_limit_bytes=40 * 2**20
            ),
            cost_estimate=pl.CostEstimate(
                flops=6 * rows * model_width * hidden_width,
                transcendentals=rows * hidden_width,
                bytes_accessed=6 * model_width * hidden_width + 4 * rows * model_width,
            ),
            name="expert",
        )(*inputs, w_gate[0], w_up[0], w_down[0])
        added = swap(part_other, "tp", 1)

        def summed(j):
            here = slice(j * each, (j + 1) * each)
            return part_mine[here].astype(jnp.float32) + added[here].astype(jnp.float32)

        result = summed(0)
        for j in range(1, blocks):
            sent = swap(summed(j).astype(jnp.bfloat16), "tp", 2 * j)
            result = result + sent.astype(jnp.float32)
        returned.append(
            lax.all_to_all(result.astype(jnp.bfloat16), "sp", 0, 0, tiled=True)
        )

    def combine(*refs):
        combine_kernel(n_sp, *refs)

    return pl.pallas_call(
        combine,
        out_shape=jax.ShapeDtypeStruct((local_rows, model_width), jnp.bfloat16),
        in_specs=[vmem] * (3 + CHUNKS),
        out_specs=vmem,
        scratch_shapes=[pltpu.VMEM((n_sp * capacity, model_width), jnp.bfloat16)],
        compiler_params=pltpu.CompilerParams(vmem_limit_bytes=24 * 2**20),
        name="combine",
    )(stream, routes, route_weights, *returned)


def solution(mesh):
    in_specs = (
        P("sp", "tp"),
        P("sp", "tp"),
        P("sp", "tp"),
        P("sp", "tp"),
        P("sp"),
        P("tp"),
        P(),
        P(("sp", "tp"), None),
        P(),
        P(("sp", "tp"), None),
        P(("sp", "tp"), None),
        P("sp", None, "tp"),
        P("sp", None, "tp"),
        P("sp", "tp", None),
    )
    out_specs = P(("sp", "tp"), None)


    return jax.shard_map(on_device, mesh=mesh, in_specs=in_specs, out_specs=out_specs, check_vma=False)
```

```python
import jax
import jax.numpy as jnp
from jax import lax
from jax.experimental import pallas as pl
from jax.experimental.pallas import tpu as pltpu
from jax.sharding import PartitionSpec as P

EPS = 1e-06
LOG2E = 1.4426950408889634
NEG = -1e30


def bf16_parts(x):
    hi = lax.reduce_precision(x, 8, 7)
    rest = x - hi
    mid = lax.reduce_precision(rest, 8, 7)
    low = rest - mid
    return [part.astype(jnp.bfloat16) for part in (hi, mid, low)]


def attention_kernel(tokens, heads, head_size, tile, sources, first, last, *refs):
    valid_ref, docs_ref, q_ref, meta_ref, gain_ref = refs[:5]
    kv_refs = refs[5 : 5 + 2 * sources]
    rest = refs[5 + 2 * sources :]
    if not first:
        m_in, l_in, acc_in, *rest = rest
    if last:
        out_ref, m_ref, l_ref, acc_ref = rest
    else:
        m_out, l_out, acc_out, m_ref, l_ref, acc_ref = rest
    width = heads * head_size
    halves = tokens // width
    rows = tokens // head_size
    score_scale = head_size ** (-0.5) * LOG2E
    lane = lax.broadcasted_iota(jnp.int32, (1, width), 1)
    in_head = [(lane >= h * head_size) & (lane < (h + 1) * head_size) for h in range(heads)]

    def spread(parts):
        full = jnp.broadcast_to(parts[0], (tile, width))
        for h in range(1, heads):
            full = jnp.where(in_head[h], parts[h], full)
        return full

    def q_tile(step, carry):
        row0 = pl.multiple_of(step * tile, tile)
        q = q_ref[pl.ds(row0, tile), :]
        meta = meta_ref[pl.ds(row0, tile), :]
        q_doc = meta[:, heads : heads + 1]
        first_doc = docs_ref[row0].astype(jnp.float32)

        def visit(source):
            fresh = first and source == 0
            k_ref, v_ref = kv_refs[2 * source], kv_refs[2 * source + 1]
            k = k_ref[:tokens, :]
            v = v_ref[...]
            extra = k_ref[tokens:, :].astype(jnp.float32)
            gates = (extra[:rows] + extra[rows : 2 * rows] + extra[2 * rows : 3 * rows]) * LOG2E
            doc_rows = extra[3 * rows : 3 * rows + halves]
            k_doc = jnp.concatenate([doc_rows[j : j + 1] for j in range(halves)], axis=1)
            allowed = k_doc == q_doc
            if fresh:
                q_pos = row0 + lax.broadcasted_iota(jnp.int32, (tile, tokens), 0)
                k_pos = lax.broadcasted_iota(jnp.int32, (tile, tokens), 1)
                allowed = allowed & (k_pos <= q_pos)
            total = jnp.zeros((tile, width), jnp.float32)
            rescales = []
            for h in range(heads):
                q_h = jnp.where(in_head[h], q, jnp.zeros((), q.dtype))
                s = lax.dot_general(
                    q_h, k, (((1,), (1,)), ((), ())), preferred_element_type=jnp.float32
                )
                gate_row = jnp.concatenate(
                    [gates[h * halves + j : h * halves + j + 1] for j in range(halves)], axis=1
                )
                s = s * score_scale + (meta[:, h : h + 1] * LOG2E - gate_row)
                s = jnp.where(allowed, s, NEG)
                block_max = jnp.max(s, axis=1, keepdims=True)
                if fresh:
                    new_max = block_max
                else:
                    old_max = m_ref[h]
                    new_max = jnp.maximum(old_max, block_max)
                    rescale = jnp.exp2(old_max - new_max)
                    rescales.append(rescale)
                p = jnp.exp2(s - new_max)
                block_sum = jnp.sum(p, axis=1, keepdims=True)
                m_ref[h] = new_max
                l_ref[h] = block_sum if fresh else l_ref[h] * rescale + block_sum
                v_h = jnp.where(in_head[h], v, jnp.zeros((), v.dtype))
                total = total + jnp.dot(
                    p.astype(jnp.bfloat16), v_h, preferred_element_type=jnp.float32
                )
            if fresh:
                acc_ref[...] = total
            else:
                acc_ref[...] = acc_ref[...] * spread(rescales) + total

        if first:
            visit(0)
        else:
            for h in range(heads):
                m_ref[h] = m_in[pl.ds(row0, tile), h : h + 1]
                l_ref[h] = l_in[pl.ds(row0, tile), h : h + 1]
            acc_ref[...] = acc_in[pl.ds(row0, tile), :]
        for source in range(1 if first else 0, sources):
            last_doc = jnp.max(
                kv_refs[2 * source][tokens + 3 * rows : tokens + 3 * rows + halves, :].astype(
                    jnp.float32
                )
            )

            @pl.when((valid_ref[source] > 0) & (last_doc >= first_doc))
            def _():
                visit(source)

        if not last:
            for h in range(heads):
                m_out[pl.ds(row0, tile), h : h + 1] = m_ref[h]
                l_out[pl.ds(row0, tile), h : h + 1] = l_ref[h]
            acc_out[pl.ds(row0, tile), :] = acc_ref[...]
            return carry

        attended = acc_ref[...] / spread([l_ref[h] for h in range(heads)])
        squares = attended * attended
        means = [
            jnp.sum(jnp.where(in_head[h], squares, 0.0), axis=1, keepdims=True) / head_size
            for h in range(heads)
        ]
        scale = spread([lax.rsqrt(mean + EPS) for mean in means])
        out_ref[pl.ds(row0, tile), :] = (attended * scale * gain_ref[...]).astype(jnp.bfloat16)
        return carry

    lax.fori_loop(0, tokens // tile, q_tile, 0)


def attend(queries, keys, values, cum_gate, documents, head_gain):
    tokens, width = queries.shape
    heads = cum_gate.shape[1]
    head_size = width // heads
    n_sp = lax.axis_size("sp")
    place = lax.axis_index("sp")
    tile = tokens // 2

    gate_rows = [part.T.reshape(-1, width) for part in bf16_parts(cum_gate)]
    doc_rows = documents.astype(jnp.bfloat16).reshape(-1, width)
    used = sum(part.shape[0] for part in gate_rows) + doc_rows.shape[0]
    filler = jnp.zeros((-used % 16, width), jnp.bfloat16)
    keys_more = jnp.concatenate([keys, *gate_rows, doc_rows, filler], axis=0)
    meta = jnp.concatenate(
        [
            cum_gate,
            documents.astype(jnp.float32)[:, None],
            jnp.zeros((tokens, 8 - (heads + 1) % 8), jnp.float32),
        ],
        axis=1,
    )

    reach = n_sp // 4
    ahead = [(i, i + 2) for i in range(n_sp - 2)]
    even_up = [(i, i + 1) for i in range(0, n_sp, 2)]
    odd_down = [(i + 1, i) for i in range(0, n_sp, 2)]

    def chain(first):
        own, other = [first], []
        for step in range(reach + 1):
            pairs = even_up if step == 0 else odd_down if step == reach else even_up + odd_down
            if step > 0:
                own.append(lax.ppermute(own[-1], "sp", ahead))
            other.append(lax.ppermute(own[-1], "sp", pairs))
        return own, other

    key_own, key_other = chain(keys_more)
    value_own, value_other = chain(values)
    group, member = place // 2, place % 2
    blocks, valid = [], []
    for step in range(reach + 1):
        exists = group - step >= 0
        blocks += [key_own[step], value_own[step]]
        valid.append(exists)
        blocks += [key_other[step], value_other[step]]
        if step == 0:
            exists = exists & (member == 1)
        elif step == reach:
            exists = exists & (member == 0)
        valid.append(exists)
    vmem = pl.BlockSpec(memory_space=pltpu.VMEM)
    smem = pl.BlockSpec(memory_space=pltpu.SMEM)
    state = [
        jax.ShapeDtypeStruct((tokens, heads), jnp.float32),
        jax.ShapeDtypeStruct((tokens, heads), jnp.float32),
        jax.ShapeDtypeStruct((tokens, width), jnp.float32),
    ]

    def run(places, carried, first, last):
        flags = jnp.stack([valid[i] for i in places]).astype(jnp.int32)
        pieces = [x for i in places for x in blocks[2 * i : 2 * i + 2]]

        def kernel(*refs):
            attention_kernel(tokens, heads, head_size, tile, len(places), first, last, *refs)

        return pl.pallas_call(
            kernel,
            out_shape=[jax.ShapeDtypeStruct((tokens, width), jnp.bfloat16)] if last else state,
            in_specs=[smem, smem] + [vmem] * (3 + len(pieces) + len(carried)),
            out_specs=[vmem] if last else [vmem] * 3,
            scratch_shapes=[
                pltpu.VMEM((heads, tile, 1), jnp.float32),
                pltpu.VMEM((heads, tile, 1), jnp.float32),
                pltpu.VMEM((tile, width), jnp.float32),
            ],
            compiler_params=pltpu.CompilerParams(vmem_limit_bytes=40 * 2**20),
            name="attention",
        )(flags, documents, queries, meta, head_gain[None, :], *pieces, *carried)

    early, late = list(range(len(valid) - 1)), [len(valid) - 1]
    carried = run(early, [], True, False)
    return run(late, carried, False, True)[0]


def swap(x, axis, bits):
    return lax.ppermute(x, axis, [(i, i ^ bits) for i in range(lax.axis_size(axis))])


def chunk_count(n_sp):
    return 4 if n_sp <= 8 else 2


def project_kernel(chunks, experts, capacity, x_ref, weight_ref, resid_ref, routes_ref, gain_ref, *refs):
    outs = refs[:chunks]
    stream_ref, wide_ref, pick_ref = refs[chunks:]
    rows, width = resid_ref.shape
    n_tile = 512
    total = jnp.zeros((rows, 1), jnp.float32)
    for n in range(width // n_tile):
        cols = slice(n * n_tile, (n + 1) * n_tile)
        projected = jnp.dot(x_ref[...], weight_ref[:, cols], preferred_element_type=jnp.float32)
        stream = (resid_ref[:, cols].astype(jnp.float32) + projected).astype(jnp.bfloat16)
        stream_ref[:, cols] = stream
        wide = stream.astype(jnp.float32)
        wide_ref[:, cols] = wide
        total = total + jnp.sum(wide * wide, axis=1, keepdims=True)
    scale = lax.rsqrt(total / width + EPS)

    before = (
        lax.broadcasted_iota(jnp.int32, (rows, rows), 0)
        < lax.broadcasted_iota(jnp.int32, (rows, rows), 1)
    ).astype(jnp.bfloat16)
    expert_ids = lax.broadcasted_iota(jnp.int32, (experts, rows), 0).astype(jnp.float32)
    chosen = jnp.zeros((experts, rows), jnp.float32)
    for route in range(2):
        chosen = chosen + (routes_ref[route : route + 1, :] == expert_ids).astype(jnp.float32)
    ranks = jnp.dot(chosen.astype(jnp.bfloat16), before, preferred_element_type=jnp.float32)
    slots = jnp.where(chosen > 0.0, ranks, -1.0)
    span = capacity // chunks
    for c in range(chunks):
        slot_ids = lax.broadcasted_iota(jnp.int32, (span, rows), 0) + c * span
        for e in range(experts):
            pick = (slot_ids.astype(jnp.float32) == slots[e : e + 1, :]).astype(jnp.float32)
            first = (c * experts + e) * span
            pick_ref[first : first + span, :] = pick
    each = experts * span
    picks = pick_ref[...].astype(jnp.bfloat16)
    for n in range(width // n_tile):
        cols = slice(n * n_tile, (n + 1) * n_tile)
        normed = (wide_ref[:, cols] * scale * gain_ref[:, cols]).astype(jnp.bfloat16)
        picked = jnp.dot(picks, normed, preferred_element_type=jnp.float32).astype(jnp.bfloat16)
        for c in range(chunks):
            outs[c][:, cols] = picked[c * each : (c + 1) * each]


def expert_kernel(count, *refs):
    inputs = refs[:count]
    gate_ref, up_ref, down_hbm = refs[count : count + 3]
    mine_ref, other_ref, x_ref, hidden_ref, down_ref, sem = refs[count + 3 :]
    mine_rows = mine_ref.shape[0]
    step, steps = pl.program_id(0), hidden_ref.shape[0]
    fetch = pltpu.make_async_copy(down_hbm, down_ref, sem)

    @pl.when(step == 0)
    def _():
        fetch.start()
        row = 0
        for ref in inputs:
            x_ref[row : row + ref.shape[0], :] = ref[...]
            row += ref.shape[0]

    both = jnp.concatenate([gate_ref[...], up_ref[...]], axis=1)
    product = jnp.dot(x_ref[...], both, preferred_element_type=jnp.float32)
    half = product.shape[1] // 2
    gate, up = product[:, :half], product[:, half:]
    hidden_ref[step] = (gate * (1.0 / (1.0 + jnp.exp(-gate))) * up).astype(jnp.bfloat16)

    @pl.when(step == steps - 1)
    def _():
        fetch.wait()
        hidden = jnp.concatenate([hidden_ref[i] for i in range(steps)], axis=1)
        n_tile = 512
        for n in range(down_ref.shape[1] // n_tile):
            cols = slice(n * n_tile, (n + 1) * n_tile)
            out = jnp.dot(
                hidden, down_ref[:, cols], preferred_element_type=jnp.float32
            ).astype(jnp.bfloat16)
            mine_ref[:, cols] = out[:mine_rows]
            other_ref[:, cols] = out[mine_rows:]


def combine_kernel(chunks, experts, stream_ref, routes_ref, weights_ref, *refs):
    outs = refs[:chunks]
    mixed_ref, stack_ref = refs[chunks:]
    rows, width = stream_ref.shape
    each = outs[0].shape[0]
    span = each // experts
    for c in range(chunks):
        stack_ref[c * each : (c + 1) * each, :] = outs[c][...]
    expert_ids = lax.broadcasted_iota(jnp.int32, (rows, experts), 1)
    named = [
        (routes_ref[:, route : route + 1] == expert_ids).astype(jnp.float32) for route in range(2)
    ]
    before = (
        lax.broadcasted_iota(jnp.int32, (rows, rows), 1)
        < lax.broadcasted_iota(jnp.int32, (rows, rows), 0)
    ).astype(jnp.bfloat16)
    ranks = jnp.dot(
        before, (named[0] + named[1]).astype(jnp.bfloat16), preferred_element_type=jnp.float32
    )
    slot_ids = lax.broadcasted_iota(jnp.int32, (rows, chunks * each), 1)
    picks = []
    for route in range(2):
        rank = jnp.sum(named[route] * ranks, axis=1, keepdims=True).astype(jnp.int32)
        chunk = rank // span
        target = chunk * each + routes_ref[:, route : route + 1] * span + (rank - chunk * span)
        picks.append((slot_ids == target).astype(jnp.float32).astype(jnp.bfloat16))
    n_tile = 512
    for n in range(width // n_tile):
        cols = slice(n * n_tile, (n + 1) * n_tile)
        mixed = stream_ref[:, cols].astype(jnp.float32)
        for route in range(2):
            result = jnp.dot(picks[route], stack_ref[:, cols], preferred_element_type=jnp.float32)
            mixed = mixed + weights_ref[:, route : route + 1] * result
        mixed_ref[:, cols] = mixed.astype(jnp.bfloat16)


def on_device(
    queries,
    keys,
    values,
    cum_gate,
    documents,
    head_gain,
    out_weight,
    resid,
    norm_gain,
    routes,
    route_weights,
    w_gate,
    w_up,
    w_down,
):
    tokens = queries.shape[0]
    n_sp, n_tp = lax.axis_size("sp"), lax.axis_size("tp")
    blocks = n_tp // 2
    local_rows, model_width = resid.shape
    capacity = 2 * routes.shape[1] * tokens // (n_tp * n_sp)
    chunks = chunk_count(n_sp)
    span = capacity // chunks
    vmem = pl.BlockSpec(memory_space=pltpu.VMEM)
    route_rows = routes.T.astype(jnp.float32)

    head_normed = attend(queries, keys, values, cum_gate, documents, head_gain)
    regrouped = lax.all_to_all(head_normed, "tp", split_axis=0, concat_axis=1, tiled=True)

    def project(*refs):
        project_kernel(chunks, n_sp, capacity, *refs)

    *outbound, stream = pl.pallas_call(
        project,
        out_shape=[jax.ShapeDtypeStruct((n_sp * span, model_width), jnp.bfloat16)] * chunks
        + [jax.ShapeDtypeStruct((local_rows, model_width), jnp.bfloat16)],
        in_specs=[vmem] * 5,
        out_specs=[vmem] * (chunks + 1),
        scratch_shapes=[
            pltpu.VMEM((local_rows, model_width), jnp.float32),
            pltpu.VMEM((n_sp * capacity, local_rows), jnp.float32),
        ],
        compiler_params=pltpu.CompilerParams(vmem_limit_bytes=40 * 2**20),
        name="project",
    )(regrouped, out_weight, resid, route_rows, norm_gain[None, :])

    hidden_width = w_gate.shape[2]
    h_tile = 128
    each = n_sp * span
    rows = n_tp * each
    arrived, crossed = [], []
    for c in range(chunks):
        arrived.append(lax.all_to_all(outbound[c], "sp", 0, 0, tiled=True))
        crossed.append([swap(arrived[c], "tp", 2 * j) for j in range(1, blocks)])
    returned = []
    for c in range(chunks):
        inputs = [arrived[c], *crossed[c]]
        inputs += [swap(x, "tp", 1) for x in inputs]

        def expert(*refs):
            expert_kernel(n_tp, *refs)

        part_mine, part_other = pl.pallas_call(
            expert,
            grid=(hidden_width // h_tile,),
            out_shape=[jax.ShapeDtypeStruct((rows // 2, model_width), jnp.bfloat16)] * 2,
            in_specs=[pl.BlockSpec(x.shape, lambda f: (0, 0)) for x in inputs]
            + [pl.BlockSpec((model_width, h_tile), lambda f: (0, f))] * 2
            + [pl.BlockSpec(memory_space=pl.ANY)],
            out_specs=[pl.BlockSpec((rows // 2, model_width), lambda f: (0, 0))] * 2,
            scratch_shapes=[
                pltpu.VMEM((rows, model_width), jnp.bfloat16),
                pltpu.VMEM((hidden_width // h_tile, rows, h_tile), jnp.bfloat16),
                pltpu.VMEM((hidden_width, model_width), jnp.bfloat16),
                pltpu.SemaphoreType.DMA,
            ],
            compiler_params=pltpu.CompilerParams(
                dimension_semantics=("arbitrary",), vmem_limit_bytes=40 * 2**20
            ),
            cost_estimate=pl.CostEstimate(
                flops=6 * rows * model_width * hidden_width,
                transcendentals=rows * hidden_width,
                bytes_accessed=6 * model_width * hidden_width + 4 * rows * model_width,
            ),
            name="expert",
        )(*inputs, w_gate[0], w_up[0], w_down[0])
        added = swap(part_other, "tp", 1)

        def summed(j):
            here = slice(j * each, (j + 1) * each)
            return part_mine[here].astype(jnp.float32) + added[here].astype(jnp.float32)

        result = summed(0)
        for j in range(1, blocks):
            sent = swap(summed(j).astype(jnp.bfloat16), "tp", 2 * j)
            result = result + sent.astype(jnp.float32)
        returned.append(
            lax.all_to_all(result.astype(jnp.bfloat16), "sp", 0, 0, tiled=True)
        )

    def combine(*refs):
        combine_kernel(chunks, n_sp, *refs)

    return pl.pallas_call(
        combine,
        out_shape=jax.ShapeDtypeStruct((local_rows, model_width), jnp.bfloat16),
        in_specs=[vmem] * (3 + chunks),
        out_specs=vmem,
        scratch_shapes=[pltpu.VMEM((n_sp * capacity, model_width), jnp.bfloat16)],
        compiler_params=pltpu.CompilerParams(vmem_limit_bytes=24 * 2**20),
        name="combine",
    )(stream, routes, route_weights, *returned)


def solution(mesh):
    in_specs = (
        P("sp", "tp"),
        P("sp", "tp"),
        P("sp", "tp"),
        P("sp", "tp"),
        P("sp"),
        P("tp"),
        P(),
        P(("sp", "tp"), None),
        P(),
        P(("sp", "tp"), None),
        P(("sp", "tp"), None),
        P("sp", None, "tp"),
        P("sp", None, "tp"),
        P("sp", "tp", None),
    )
    out_specs = P(("sp", "tp"), None)


    return jax.shard_map(on_device, mesh=mesh, in_specs=in_specs, out_specs=out_specs, check_vma=False)
```

```python
import jax
import jax.numpy as jnp
from jax import lax
from jax.experimental import pallas as pl
from jax.experimental.pallas import tpu as pltpu
from jax.sharding import PartitionSpec as P

EPS = 1e-06
LOG2E = 1.4426950408889634
NEG = -1e30


def bf16_parts(x):
    hi = lax.reduce_precision(x, 8, 7)
    rest = x - hi
    mid = lax.reduce_precision(rest, 8, 7)
    low = rest - mid
    return [part.astype(jnp.bfloat16) for part in (hi, mid, low)]


def attention_kernel(tokens, heads, head_size, tile, sources, *refs):
    valid_ref, docs_ref, q_ref, meta_ref, gain_ref = refs[:5]
    kv_refs = refs[5 : 5 + 2 * sources]
    out_ref, m_ref, l_ref, acc_ref = refs[5 + 2 * sources :]
    width = heads * head_size
    halves = tokens // width
    rows = tokens // head_size
    score_scale = head_size ** (-0.5) * LOG2E
    lane = lax.broadcasted_iota(jnp.int32, (1, width), 1)
    in_head = [(lane >= h * head_size) & (lane < (h + 1) * head_size) for h in range(heads)]

    def spread(parts):
        full = jnp.broadcast_to(parts[0], (tile, width))
        for h in range(1, heads):
            full = jnp.where(in_head[h], parts[h], full)
        return full

    def q_tile(step, carry):
        row0 = pl.multiple_of(step * tile, tile)
        q = q_ref[pl.ds(row0, tile), :]
        meta = meta_ref[pl.ds(row0, tile), :]
        q_doc = meta[:, heads : heads + 1]
        first_doc = docs_ref[row0].astype(jnp.float32)

        def visit(source):
            k_ref, v_ref = kv_refs[2 * source], kv_refs[2 * source + 1]
            k = k_ref[:tokens, :]
            v = v_ref[...]
            extra = k_ref[tokens:, :].astype(jnp.float32)
            gates = (extra[:rows] + extra[rows : 2 * rows] + extra[2 * rows : 3 * rows]) * LOG2E
            doc_rows = extra[3 * rows : 3 * rows + halves]
            k_doc = jnp.concatenate([doc_rows[j : j + 1] for j in range(halves)], axis=1)
            allowed = k_doc == q_doc
            if source == 0:
                q_pos = row0 + lax.broadcasted_iota(jnp.int32, (tile, tokens), 0)
                k_pos = lax.broadcasted_iota(jnp.int32, (tile, tokens), 1)
                allowed = allowed & (k_pos <= q_pos)
            total = jnp.zeros((tile, width), jnp.float32)
            rescales = []
            for h in range(heads):
                q_h = jnp.where(in_head[h], q, jnp.zeros((), q.dtype))
                s = lax.dot_general(
                    q_h, k, (((1,), (1,)), ((), ())), preferred_element_type=jnp.float32
                )
                gate_row = jnp.concatenate(
                    [gates[h * halves + j : h * halves + j + 1] for j in range(halves)], axis=1
                )
                s = s * score_scale + (meta[:, h : h + 1] * LOG2E - gate_row)
                s = jnp.where(allowed, s, NEG)
                block_max = jnp.max(s, axis=1, keepdims=True)
                if source == 0:
                    new_max = block_max
                else:
                    old_max = m_ref[h]
                    new_max = jnp.maximum(old_max, block_max)
                    rescale = jnp.exp2(old_max - new_max)
                    rescales.append(rescale)
                p = jnp.exp2(s - new_max)
                block_sum = jnp.sum(p, axis=1, keepdims=True)
                m_ref[h] = new_max
                l_ref[h] = block_sum if source == 0 else l_ref[h] * rescale + block_sum
                v_h = jnp.where(in_head[h], v, jnp.zeros((), v.dtype))
                total = total + jnp.dot(
                    p.astype(jnp.bfloat16), v_h, preferred_element_type=jnp.float32
                )
            if source == 0:
                acc_ref[...] = total
            else:
                acc_ref[...] = acc_ref[...] * spread(rescales) + total

        visit(0)
        for source in range(1, sources):
            last_doc = jnp.max(
                kv_refs[2 * source][tokens + 3 * rows : tokens + 3 * rows + halves, :].astype(
                    jnp.float32
                )
            )

            @pl.when((valid_ref[source] > 0) & (last_doc >= first_doc))
            def _():
                visit(source)

        attended = acc_ref[...] / spread([l_ref[h] for h in range(heads)])
        squares = attended * attended
        means = [
            jnp.sum(jnp.where(in_head[h], squares, 0.0), axis=1, keepdims=True) / head_size
            for h in range(heads)
        ]
        scale = spread([lax.rsqrt(mean + EPS) for mean in means])
        out_ref[pl.ds(row0, tile), :] = (attended * scale * gain_ref[...]).astype(jnp.bfloat16)
        return carry

    lax.fori_loop(0, tokens // tile, q_tile, 0)


def attend(queries, keys, values, cum_gate, documents, head_gain):
    tokens, width = queries.shape
    heads = cum_gate.shape[1]
    head_size = width // heads
    n_sp = lax.axis_size("sp")
    place = lax.axis_index("sp")
    tile = tokens // 2

    gate_rows = [part.T.reshape(-1, width) for part in bf16_parts(cum_gate)]
    doc_rows = documents.astype(jnp.bfloat16).reshape(-1, width)
    used = sum(part.shape[0] for part in gate_rows) + doc_rows.shape[0]
    filler = jnp.zeros((-used % 16, width), jnp.bfloat16)
    keys_more = jnp.concatenate([keys, *gate_rows, doc_rows, filler], axis=0)
    meta = jnp.concatenate(
        [
            cum_gate,
            documents.astype(jnp.float32)[:, None],
            jnp.zeros((tokens, 8 - (heads + 1) % 8), jnp.float32),
        ],
        axis=1,
    )

    reach = n_sp // 4
    ahead = [(i, i + 2) for i in range(n_sp - 2)]
    even_up = [(i, i + 1) for i in range(0, n_sp, 2)]
    odd_down = [(i + 1, i) for i in range(0, n_sp, 2)]

    def chain(first):
        own, other = [first], []
        for step in range(reach + 1):
            pairs = even_up if step == 0 else odd_down if step == reach else even_up + odd_down
            if step > 0:
                own.append(lax.ppermute(own[-1], "sp", ahead))
            other.append(lax.ppermute(own[-1], "sp", pairs))
        return own, other

    key_own, key_other = chain(keys_more)
    value_own, value_other = chain(values)
    group, member = place // 2, place % 2
    blocks, valid = [], []
    for step in range(reach + 1):
        exists = group - step >= 0
        blocks += [key_own[step], value_own[step]]
        valid.append(exists)
        blocks += [key_other[step], value_other[step]]
        if step == 0:
            exists = exists & (member == 1)
        elif step == reach:
            exists = exists & (member == 0)
        valid.append(exists)
    sources = len(valid)
    valid = jnp.stack(valid).astype(jnp.int32)

    def kernel(*refs):
        attention_kernel(tokens, heads, head_size, tile, sources, *refs)

    vmem = pl.BlockSpec(memory_space=pltpu.VMEM)
    smem = pl.BlockSpec(memory_space=pltpu.SMEM)
    return pl.pallas_call(
        kernel,
        out_shape=jax.ShapeDtypeStruct((tokens, width), jnp.bfloat16),
        in_specs=[smem, smem] + [vmem] * (3 + len(blocks)),
        out_specs=vmem,
        scratch_shapes=[
            pltpu.VMEM((heads, tile, 1), jnp.float32),
            pltpu.VMEM((heads, tile, 1), jnp.float32),
            pltpu.VMEM((tile, width), jnp.float32),
        ],
        compiler_params=pltpu.CompilerParams(vmem_limit_bytes=50 * 2**20),
        name="attention",
    )(valid, documents, queries, meta, head_gain[None, :], *blocks)


def swap(x, axis, bits):
    return lax.ppermute(x, axis, [(i, i ^ bits) for i in range(lax.axis_size(axis))])


CHUNKS = 2


def project_kernel(experts, capacity, x_ref, weight_ref, resid_ref, routes_ref, gain_ref, *refs):
    outs = refs[:CHUNKS]
    stream_ref, wide_ref, pick_ref = refs[CHUNKS:]
    rows, width = resid_ref.shape
    n_tile = 512
    total = jnp.zeros((rows, 1), jnp.float32)
    for n in range(width // n_tile):
        cols = slice(n * n_tile, (n + 1) * n_tile)
        projected = jnp.dot(x_ref[...], weight_ref[:, cols], preferred_element_type=jnp.float32)
        stream = (resid_ref[:, cols].astype(jnp.float32) + projected).astype(jnp.bfloat16)
        stream_ref[:, cols] = stream
        wide = stream.astype(jnp.float32)
        wide_ref[:, cols] = wide
        total = total + jnp.sum(wide * wide, axis=1, keepdims=True)
    scale = lax.rsqrt(total / width + EPS)

    before = (
        lax.broadcasted_iota(jnp.int32, (rows, rows), 0)
        < lax.broadcasted_iota(jnp.int32, (rows, rows), 1)
    ).astype(jnp.bfloat16)
    expert_ids = lax.broadcasted_iota(jnp.int32, (experts, rows), 0).astype(jnp.float32)
    chosen = jnp.zeros((experts, rows), jnp.float32)
    for route in range(2):
        chosen = chosen + (routes_ref[route : route + 1, :] == expert_ids).astype(jnp.float32)
    ranks = jnp.dot(chosen.astype(jnp.bfloat16), before, preferred_element_type=jnp.float32)
    slots = jnp.where(chosen > 0.0, ranks, -1.0)
    span = capacity // CHUNKS
    for c in range(CHUNKS):
        slot_ids = lax.broadcasted_iota(jnp.int32, (span, rows), 0) + c * span
        for e in range(experts):
            pick = (slot_ids.astype(jnp.float32) == slots[e : e + 1, :]).astype(jnp.float32)
            first = (c * experts + e) * span
            pick_ref[first : first + span, :] = pick
    each = experts * span
    picks = pick_ref[...].astype(jnp.bfloat16)
    for n in range(width // n_tile):
        cols = slice(n * n_tile, (n + 1) * n_tile)
        normed = (wide_ref[:, cols] * scale * gain_ref[:, cols]).astype(jnp.bfloat16)
        picked = jnp.dot(picks, normed, preferred_element_type=jnp.float32).astype(jnp.bfloat16)
        for c in range(CHUNKS):
            outs[c][:, cols] = picked[c * each : (c + 1) * each]


def expert_kernel(count, *refs):
    inputs = refs[:count]
    gate_ref, up_ref, down_hbm = refs[count : count + 3]
    mine_ref, other_ref, x_ref, hidden_ref, down_ref, sems = refs[count + 3 :]
    mine_rows = mine_ref.shape[0]
    step, steps = pl.program_id(0), hidden_ref.shape[0]
    each = x_ref.shape[0] // count
    fetch = pltpu.make_async_copy(down_hbm, down_ref, sems.at[count])
    loads = [
        pltpu.make_async_copy(ref, x_ref.at[pl.ds(i * each, each)], sems.at[i])
        for i, ref in enumerate(inputs)
    ]

    @pl.when(step == 0)
    def _():
        for load in loads:
            load.start()
        fetch.start()
        for load in loads:
            load.wait()

    both = jnp.concatenate([gate_ref[...], up_ref[...]], axis=1)
    product = jnp.dot(x_ref[...], both, preferred_element_type=jnp.float32)
    half = product.shape[1] // 2
    gate, up = product[:, :half], product[:, half:]
    hidden_ref[step] = (gate * (1.0 / (1.0 + jnp.exp(-gate))) * up).astype(jnp.bfloat16)

    @pl.when(step == steps - 1)
    def _():
        fetch.wait()
        hidden = jnp.concatenate([hidden_ref[i] for i in range(steps)], axis=1)
        n_tile = 512
        for n in range(down_ref.shape[1] // n_tile):
            cols = slice(n * n_tile, (n + 1) * n_tile)
            out = jnp.dot(
                hidden, down_ref[:, cols], preferred_element_type=jnp.float32
            ).astype(jnp.bfloat16)
            mine_ref[:, cols] = out[:mine_rows]
            other_ref[:, cols] = out[mine_rows:]


def combine_kernel(experts, stream_ref, routes_ref, weights_ref, *refs):
    outs = refs[:CHUNKS]
    mixed_ref, stack_ref = refs[CHUNKS:]
    rows, width = stream_ref.shape
    each = outs[0].shape[0]
    span = each // experts
    for c in range(CHUNKS):
        stack_ref[c * each : (c + 1) * each, :] = outs[c][...]
    expert_ids = lax.broadcasted_iota(jnp.int32, (rows, experts), 1)
    named = [
        (routes_ref[:, route : route + 1] == expert_ids).astype(jnp.float32) for route in range(2)
    ]
    before = (
        lax.broadcasted_iota(jnp.int32, (rows, rows), 1)
        < lax.broadcasted_iota(jnp.int32, (rows, rows), 0)
    ).astype(jnp.bfloat16)
    ranks = jnp.dot(
        before, (named[0] + named[1]).astype(jnp.bfloat16), preferred_element_type=jnp.float32
    )
    slot_ids = lax.broadcasted_iota(jnp.int32, (rows, CHUNKS * each), 1)
    picks = []
    for route in range(2):
        rank = jnp.sum(named[route] * ranks, axis=1, keepdims=True).astype(jnp.int32)
        chunk = rank // span
        target = chunk * each + routes_ref[:, route : route + 1] * span + (rank - chunk * span)
        picks.append((slot_ids == target).astype(jnp.float32).astype(jnp.bfloat16))
    n_tile = 512
    for n in range(width // n_tile):
        cols = slice(n * n_tile, (n + 1) * n_tile)
        mixed = stream_ref[:, cols].astype(jnp.float32)
        for route in range(2):
            result = jnp.dot(picks[route], stack_ref[:, cols], preferred_element_type=jnp.float32)
            mixed = mixed + weights_ref[:, route : route + 1] * result
        mixed_ref[:, cols] = mixed.astype(jnp.bfloat16)


def on_device(
    queries,
    keys,
    values,
    cum_gate,
    documents,
    head_gain,
    out_weight,
    resid,
    norm_gain,
    routes,
    route_weights,
    w_gate,
    w_up,
    w_down,
):
    tokens = queries.shape[0]
    n_sp, n_tp = lax.axis_size("sp"), lax.axis_size("tp")
    blocks = n_tp // 2
    local_rows, model_width = resid.shape
    capacity = 2 * routes.shape[1] * tokens // (n_tp * n_sp)
    span = capacity // CHUNKS
    vmem = pl.BlockSpec(memory_space=pltpu.VMEM)
    route_rows = routes.T.astype(jnp.float32)

    head_normed = attend(queries, keys, values, cum_gate, documents, head_gain)
    regrouped = lax.all_to_all(head_normed, "tp", split_axis=0, concat_axis=1, tiled=True)

    def project(*refs):
        project_kernel(n_sp, capacity, *refs)

    *outbound, stream = pl.pallas_call(
        project,
        out_shape=[jax.ShapeDtypeStruct((n_sp * span, model_width), jnp.bfloat16)] * CHUNKS
        + [jax.ShapeDtypeStruct((local_rows, model_width), jnp.bfloat16)],
        in_specs=[vmem] * 5,
        out_specs=[vmem] * (CHUNKS + 1),
        scratch_shapes=[
            pltpu.VMEM((local_rows, model_width), jnp.float32),
            pltpu.VMEM((n_sp * capacity, local_rows), jnp.float32),
        ],
        compiler_params=pltpu.CompilerParams(vmem_limit_bytes=40 * 2**20),
        name="project",
    )(regrouped, out_weight, resid, route_rows, norm_gain[None, :])

    hidden_width = w_gate.shape[2]
    h_tile = 128
    each = n_sp * span
    rows = n_tp * each
    arrived, crossed = [], []
    for c in range(CHUNKS):
        arrived.append(lax.all_to_all(outbound[c], "sp", 0, 0, tiled=True))
        crossed.append([swap(arrived[c], "tp", 2 * j) for j in range(1, blocks)])
    returned = []
    for c in range(CHUNKS):
        inputs = [arrived[c], *crossed[c]]
        inputs += [swap(x, "tp", 1) for x in inputs]

        def expert(*refs):
            expert_kernel(n_tp, *refs)

        part_mine, part_other = pl.pallas_call(
            expert,
            grid=(hidden_width // h_tile,),
            out_shape=[jax.ShapeDtypeStruct((rows // 2, model_width), jnp.bfloat16)] * 2,
            in_specs=[pl.BlockSpec(memory_space=pltpu.HBM)] * len(inputs)
            + [pl.BlockSpec((model_width, h_tile), lambda f: (0, f))] * 2
            + [pl.BlockSpec(memory_space=pl.ANY)],
            out_specs=[pl.BlockSpec((rows // 2, model_width), lambda f: (0, 0))] * 2,
            scratch_shapes=[
                pltpu.VMEM((rows, model_width), jnp.bfloat16),
                pltpu.VMEM((hidden_width // h_tile, rows, h_tile), jnp.bfloat16),
                pltpu.VMEM((hidden_width, model_width), jnp.bfloat16),
                pltpu.SemaphoreType.DMA((n_tp + 1,)),
            ],
            compiler_params=pltpu.CompilerParams(
                dimension_semantics=("arbitrary",), vmem_limit_bytes=40 * 2**20
            ),
            cost_estimate=pl.CostEstimate(
                flops=6 * rows * model_width * hidden_width,
                transcendentals=rows * hidden_width,
                bytes_accessed=6 * model_width * hidden_width + 4 * rows * model_width,
            ),
            name="expert",
        )(*inputs, w_gate[0], w_up[0], w_down[0])
        added = swap(part_other, "tp", 1)

        def summed(j):
            here = slice(j * each, (j + 1) * each)
            return part_mine[here].astype(jnp.float32) + added[here].astype(jnp.float32)

        result = summed(0)
        for j in range(1, blocks):
            sent = swap(summed(j).astype(jnp.bfloat16), "tp", 2 * j)
            result = result + sent.astype(jnp.float32)
        returned.append(
            lax.all_to_all(result.astype(jnp.bfloat16), "sp", 0, 0, tiled=True)
        )

    def combine(*refs):
        combine_kernel(n_sp, *refs)

    return pl.pallas_call(
        combine,
        out_shape=jax.ShapeDtypeStruct((local_rows, model_width), jnp.bfloat16),
        in_specs=[vmem] * (3 + CHUNKS),
        out_specs=vmem,
        scratch_shapes=[pltpu.VMEM((n_sp * capacity, model_width), jnp.bfloat16)],
        compiler_params=pltpu.CompilerParams(vmem_limit_bytes=24 * 2**20),
        name="combine",
    )(stream, routes, route_weights, *returned)


def solution(mesh):
    in_specs = (
        P("sp", "tp"),
        P("sp", "tp"),
        P("sp", "tp"),
        P("sp", "tp"),
        P("sp"),
        P("tp"),
        P(),
        P(("sp", "tp"), None),
        P(),
        P(("sp", "tp"), None),
        P(("sp", "tp"), None),
        P("sp", None, "tp"),
        P("sp", None, "tp"),
        P("sp", "tp", None),
    )
    out_specs = P(("sp", "tp"), None)


    return jax.shard_map(on_device, mesh=mesh, in_specs=in_specs, out_specs=out_specs, check_vma=False)
```

```python
import jax
import jax.numpy as jnp
from jax import lax
from jax.experimental import pallas as pl
from jax.experimental.pallas import tpu as pltpu
from jax.sharding import PartitionSpec as P

EPS = 1e-06
LOG2E = 1.4426950408889634
NEG = -1e30


def bf16_parts(x):
    hi = lax.reduce_precision(x, 8, 7)
    rest = x - hi
    mid = lax.reduce_precision(rest, 8, 7)
    low = rest - mid
    return [part.astype(jnp.bfloat16) for part in (hi, mid, low)]


def attention_kernel(tokens, heads, head_size, tile, sources, *refs):
    valid_ref, docs_ref, q_ref, meta_ref, gain_ref = refs[:5]
    kv_refs = refs[5 : 5 + 2 * sources]
    out_ref, m_ref, l_ref, acc_ref, *held, sems = refs[5 + 2 * sources :]
    loads = [
        pltpu.make_async_copy(source, target, sems.at[i])
        for i, (source, target) in enumerate(zip(kv_refs, held))
    ]
    for load in loads:
        load.start()
    kv_refs = held
    width = heads * head_size
    halves = tokens // width
    rows = tokens // head_size
    score_scale = head_size ** (-0.5) * LOG2E
    lane = lax.broadcasted_iota(jnp.int32, (1, width), 1)
    in_head = [(lane >= h * head_size) & (lane < (h + 1) * head_size) for h in range(heads)]

    def spread(parts):
        full = jnp.broadcast_to(parts[0], (tile, width))
        for h in range(1, heads):
            full = jnp.where(in_head[h], parts[h], full)
        return full

    def q_tile(step, carry):
        row0 = pl.multiple_of(step * tile, tile)
        q = q_ref[pl.ds(row0, tile), :]
        meta = meta_ref[pl.ds(row0, tile), :]
        q_doc = meta[:, heads : heads + 1]
        first_doc = docs_ref[row0].astype(jnp.float32)

        def visit(source):
            k_ref, v_ref = kv_refs[2 * source], kv_refs[2 * source + 1]
            k = k_ref[:tokens, :]
            v = v_ref[...]
            extra = k_ref[tokens:, :].astype(jnp.float32)
            gates = (extra[:rows] + extra[rows : 2 * rows] + extra[2 * rows : 3 * rows]) * LOG2E
            doc_rows = extra[3 * rows : 3 * rows + halves]
            k_doc = jnp.concatenate([doc_rows[j : j + 1] for j in range(halves)], axis=1)
            allowed = k_doc == q_doc
            if source == 0:
                q_pos = row0 + lax.broadcasted_iota(jnp.int32, (tile, tokens), 0)
                k_pos = lax.broadcasted_iota(jnp.int32, (tile, tokens), 1)
                allowed = allowed & (k_pos <= q_pos)
            total = jnp.zeros((tile, width), jnp.float32)
            rescales = []
            for h in range(heads):
                q_h = jnp.where(in_head[h], q, jnp.zeros((), q.dtype))
                s = lax.dot_general(
                    q_h, k, (((1,), (1,)), ((), ())), preferred_element_type=jnp.float32
                )
                gate_row = jnp.concatenate(
                    [gates[h * halves + j : h * halves + j + 1] for j in range(halves)], axis=1
                )
                s = s * score_scale + (meta[:, h : h + 1] * LOG2E - gate_row)
                s = jnp.where(allowed, s, NEG)
                block_max = jnp.max(s, axis=1, keepdims=True)
                if source == 0:
                    new_max = block_max
                else:
                    old_max = m_ref[h]
                    new_max = jnp.maximum(old_max, block_max)
                    rescale = jnp.exp2(old_max - new_max)
                    rescales.append(rescale)
                p = jnp.exp2(s - new_max)
                block_sum = jnp.sum(p, axis=1, keepdims=True)
                m_ref[h] = new_max
                l_ref[h] = block_sum if source == 0 else l_ref[h] * rescale + block_sum
                v_h = jnp.where(in_head[h], v, jnp.zeros((), v.dtype))
                total = total + jnp.dot(
                    p.astype(jnp.bfloat16), v_h, preferred_element_type=jnp.float32
                )
            if source == 0:
                acc_ref[...] = total
            else:
                acc_ref[...] = acc_ref[...] * spread(rescales) + total

        def arrive(source):
            @pl.when(step == 0)
            def _():
                loads[2 * source].wait()
                loads[2 * source + 1].wait()

        arrive(0)
        visit(0)
        for source in range(1, sources):
            arrive(source)
            last_doc = jnp.max(
                kv_refs[2 * source][tokens + 3 * rows : tokens + 3 * rows + halves, :].astype(
                    jnp.float32
                )
            )

            @pl.when((valid_ref[source] > 0) & (last_doc >= first_doc))
            def _():
                visit(source)

        attended = acc_ref[...] / spread([l_ref[h] for h in range(heads)])
        squares = attended * attended
        means = [
            jnp.sum(jnp.where(in_head[h], squares, 0.0), axis=1, keepdims=True) / head_size
            for h in range(heads)
        ]
        scale = spread([lax.rsqrt(mean + EPS) for mean in means])
        out_ref[pl.ds(row0, tile), :] = (attended * scale * gain_ref[...]).astype(jnp.bfloat16)
        return carry

    lax.fori_loop(0, tokens // tile, q_tile, 0)


def attend(queries, keys, values, cum_gate, documents, head_gain):
    tokens, width = queries.shape
    heads = cum_gate.shape[1]
    head_size = width // heads
    n_sp = lax.axis_size("sp")
    place = lax.axis_index("sp")
    tile = tokens // 2

    gate_rows = [part.T.reshape(-1, width) for part in bf16_parts(cum_gate)]
    doc_rows = documents.astype(jnp.bfloat16).reshape(-1, width)
    used = sum(part.shape[0] for part in gate_rows) + doc_rows.shape[0]
    filler = jnp.zeros((-used % 16, width), jnp.bfloat16)
    keys_more = jnp.concatenate([keys, *gate_rows, doc_rows, filler], axis=0)
    meta = jnp.concatenate(
        [
            cum_gate,
            documents.astype(jnp.float32)[:, None],
            jnp.zeros((tokens, 8 - (heads + 1) % 8), jnp.float32),
        ],
        axis=1,
    )

    reach = n_sp // 4
    ahead = [(i, i + 2) for i in range(n_sp - 2)]
    even_up = [(i, i + 1) for i in range(0, n_sp, 2)]
    odd_down = [(i + 1, i) for i in range(0, n_sp, 2)]

    def chain(first):
        own, other = [first], []
        for step in range(reach + 1):
            pairs = even_up if step == 0 else odd_down if step == reach else even_up + odd_down
            if step > 0:
                own.append(lax.ppermute(own[-1], "sp", ahead))
            other.append(lax.ppermute(own[-1], "sp", pairs))
        return own, other

    key_own, key_other = chain(keys_more)
    value_own, value_other = chain(values)
    group, member = place // 2, place % 2
    blocks, valid = [], []
    for step in range(reach + 1):
        exists = group - step >= 0
        blocks += [key_own[step], value_own[step]]
        valid.append(exists)
        blocks += [key_other[step], value_other[step]]
        if step == 0:
            exists = exists & (member == 1)
        elif step == reach:
            exists = exists & (member == 0)
        valid.append(exists)
    sources = len(valid)
    valid = jnp.stack(valid).astype(jnp.int32)

    def kernel(*refs):
        attention_kernel(tokens, heads, head_size, tile, sources, *refs)

    vmem = pl.BlockSpec(memory_space=pltpu.VMEM)
    smem = pl.BlockSpec(memory_space=pltpu.SMEM)
    return pl.pallas_call(
        kernel,
        out_shape=jax.ShapeDtypeStruct((tokens, width), jnp.bfloat16),
        in_specs=[smem, smem] + [vmem] * 3 + [pl.BlockSpec(memory_space=pltpu.HBM)] * len(blocks),
        out_specs=vmem,
        scratch_shapes=[
            pltpu.VMEM((heads, tile, 1), jnp.float32),
            pltpu.VMEM((heads, tile, 1), jnp.float32),
            pltpu.VMEM((tile, width), jnp.float32),
            *[pltpu.VMEM(x.shape, x.dtype) for x in blocks],
            pltpu.SemaphoreType.DMA((len(blocks),)),
        ],
        compiler_params=pltpu.CompilerParams(vmem_limit_bytes=36 * 2**20),
        name="attention",
    )(valid, documents, queries, meta, head_gain[None, :], *blocks)


def swap(x, axis, bits):
    return lax.ppermute(x, axis, [(i, i ^ bits) for i in range(lax.axis_size(axis))])


CHUNKS = 2


def project_kernel(experts, capacity, x_ref, weight_ref, resid_ref, routes_ref, gain_ref, *refs):
    outs = refs[:CHUNKS]
    stream_ref, wide_ref, pick_ref = refs[CHUNKS:]
    rows, width = resid_ref.shape
    n_tile = 512
    total = jnp.zeros((rows, 1), jnp.float32)
    for n in range(width // n_tile):
        cols = slice(n * n_tile, (n + 1) * n_tile)
        projected = jnp.dot(x_ref[...], weight_ref[:, cols], preferred_element_type=jnp.float32)
        stream = (resid_ref[:, cols].astype(jnp.float32) + projected).astype(jnp.bfloat16)
        stream_ref[:, cols] = stream
        wide = stream.astype(jnp.float32)
        wide_ref[:, cols] = wide
        total = total + jnp.sum(wide * wide, axis=1, keepdims=True)
    scale = lax.rsqrt(total / width + EPS)

    before = (
        lax.broadcasted_iota(jnp.int32, (rows, rows), 0)
        < lax.broadcasted_iota(jnp.int32, (rows, rows), 1)
    ).astype(jnp.bfloat16)
    expert_ids = lax.broadcasted_iota(jnp.int32, (experts, rows), 0).astype(jnp.float32)
    chosen = jnp.zeros((experts, rows), jnp.float32)
    for route in range(2):
        chosen = chosen + (routes_ref[route : route + 1, :] == expert_ids).astype(jnp.float32)
    ranks = jnp.dot(chosen.astype(jnp.bfloat16), before, preferred_element_type=jnp.float32)
    slots = jnp.where(chosen > 0.0, ranks, -1.0)
    span = capacity // CHUNKS
    for c in range(CHUNKS):
        slot_ids = lax.broadcasted_iota(jnp.int32, (span, rows), 0) + c * span
        for e in range(experts):
            pick = (slot_ids.astype(jnp.float32) == slots[e : e + 1, :]).astype(jnp.float32)
            first = (c * experts + e) * span
            pick_ref[first : first + span, :] = pick
    each = experts * span
    picks = pick_ref[...].astype(jnp.bfloat16)
    for n in range(width // n_tile):
        cols = slice(n * n_tile, (n + 1) * n_tile)
        normed = (wide_ref[:, cols] * scale * gain_ref[:, cols]).astype(jnp.bfloat16)
        picked = jnp.dot(picks, normed, preferred_element_type=jnp.float32).astype(jnp.bfloat16)
        for c in range(CHUNKS):
            outs[c][:, cols] = picked[c * each : (c + 1) * each]


def expert_kernel(count, *refs):
    inputs = refs[:count]
    gate_ref, up_ref, down_hbm = refs[count : count + 3]
    mine_ref, other_ref, x_ref, hidden_ref, down_ref, sems = refs[count + 3 :]
    mine_rows = mine_ref.shape[0]
    step, steps = pl.program_id(0), hidden_ref.shape[0]
    each = x_ref.shape[0] // count
    fetch = pltpu.make_async_copy(down_hbm, down_ref, sems.at[count])
    loads = [
        pltpu.make_async_copy(ref, x_ref.at[pl.ds(i * each, each)], sems.at[i])
        for i, ref in enumerate(inputs)
    ]

    @pl.when(step == 0)
    def _():
        for load in loads:
            load.start()
        fetch.start()
        for load in loads:
            load.wait()

    both = jnp.concatenate([gate_ref[...], up_ref[...]], axis=1)
    product = jnp.dot(x_ref[...], both, preferred_element_type=jnp.float32)
    half = product.shape[1] // 2
    gate, up = product[:, :half], product[:, half:]
    hidden_ref[step] = (gate * (1.0 / (1.0 + jnp.exp(-gate))) * up).astype(jnp.bfloat16)

    @pl.when(step == steps - 1)
    def _():
        fetch.wait()
        hidden = jnp.concatenate([hidden_ref[i] for i in range(steps)], axis=1)
        n_tile = 512
        for n in range(down_ref.shape[1] // n_tile):
            cols = slice(n * n_tile, (n + 1) * n_tile)
            out = jnp.dot(
                hidden, down_ref[:, cols], preferred_element_type=jnp.float32
            ).astype(jnp.bfloat16)
            mine_ref[:, cols] = out[:mine_rows]
            other_ref[:, cols] = out[mine_rows:]


def combine_kernel(experts, stream_ref, routes_ref, weights_ref, *refs):
    outs = refs[:CHUNKS]
    mixed_ref, stack_ref = refs[CHUNKS:]
    rows, width = stream_ref.shape
    each = outs[0].shape[0]
    span = each // experts
    for c in range(CHUNKS):
        stack_ref[c * each : (c + 1) * each, :] = outs[c][...]
    expert_ids = lax.broadcasted_iota(jnp.int32, (rows, experts), 1)
    named = [
        (routes_ref[:, route : route + 1] == expert_ids).astype(jnp.float32) for route in range(2)
    ]
    before = (
        lax.broadcasted_iota(jnp.int32, (rows, rows), 1)
        < lax.broadcasted_iota(jnp.int32, (rows, rows), 0)
    ).astype(jnp.bfloat16)
    ranks = jnp.dot(
        before, (named[0] + named[1]).astype(jnp.bfloat16), preferred_element_type=jnp.float32
    )
    slot_ids = lax.broadcasted_iota(jnp.int32, (rows, CHUNKS * each), 1)
    picks = []
    for route in range(2):
        rank = jnp.sum(named[route] * ranks, axis=1, keepdims=True).astype(jnp.int32)
        chunk = rank // span
        target = chunk * each + routes_ref[:, route : route + 1] * span + (rank - chunk * span)
        picks.append((slot_ids == target).astype(jnp.float32).astype(jnp.bfloat16))
    n_tile = 512
    for n in range(width // n_tile):
        cols = slice(n * n_tile, (n + 1) * n_tile)
        mixed = stream_ref[:, cols].astype(jnp.float32)
        for route in range(2):
            result = jnp.dot(picks[route], stack_ref[:, cols], preferred_element_type=jnp.float32)
            mixed = mixed + weights_ref[:, route : route + 1] * result
        mixed_ref[:, cols] = mixed.astype(jnp.bfloat16)


def on_device(
    queries,
    keys,
    values,
    cum_gate,
    documents,
    head_gain,
    out_weight,
    resid,
    norm_gain,
    routes,
    route_weights,
    w_gate,
    w_up,
    w_down,
):
    tokens = queries.shape[0]
    n_sp, n_tp = lax.axis_size("sp"), lax.axis_size("tp")
    blocks = n_tp // 2
    local_rows, model_width = resid.shape
    capacity = 2 * routes.shape[1] * tokens // (n_tp * n_sp)
    span = capacity // CHUNKS
    vmem = pl.BlockSpec(memory_space=pltpu.VMEM)
    route_rows = routes.T.astype(jnp.float32)

    head_normed = attend(queries, keys, values, cum_gate, documents, head_gain)
    regrouped = lax.all_to_all(head_normed, "tp", split_axis=0, concat_axis=1, tiled=True)

    def project(*refs):
        project_kernel(n_sp, capacity, *refs)

    *outbound, stream = pl.pallas_call(
        project,
        out_shape=[jax.ShapeDtypeStruct((n_sp * span, model_width), jnp.bfloat16)] * CHUNKS
        + [jax.ShapeDtypeStruct((local_rows, model_width), jnp.bfloat16)],
        in_specs=[vmem] * 5,
        out_specs=[vmem] * (CHUNKS + 1),
        scratch_shapes=[
            pltpu.VMEM((local_rows, model_width), jnp.float32),
            pltpu.VMEM((n_sp * capacity, local_rows), jnp.float32),
        ],
        compiler_params=pltpu.CompilerParams(vmem_limit_bytes=40 * 2**20),
        name="project",
    )(regrouped, out_weight, resid, route_rows, norm_gain[None, :])

    hidden_width = w_gate.shape[2]
    h_tile = 128
    each = n_sp * span
    rows = n_tp * each
    arrived, crossed = [], []
    for c in range(CHUNKS):
        arrived.append(lax.all_to_all(outbound[c], "sp", 0, 0, tiled=True))
        crossed.append([swap(arrived[c], "tp", 2 * j) for j in range(1, blocks)])
    returned = []
    for c in range(CHUNKS):
        inputs = [arrived[c], *crossed[c]]
        inputs += [swap(x, "tp", 1) for x in inputs]

        def expert(*refs):
            expert_kernel(n_tp, *refs)

        part_mine, part_other = pl.pallas_call(
            expert,
            grid=(hidden_width // h_tile,),
            out_shape=[jax.ShapeDtypeStruct((rows // 2, model_width), jnp.bfloat16)] * 2,
            in_specs=[pl.BlockSpec(memory_space=pltpu.HBM)] * len(inputs)
            + [pl.BlockSpec((model_width, h_tile), lambda f: (0, f))] * 2
            + [pl.BlockSpec(memory_space=pl.ANY)],
            out_specs=[pl.BlockSpec((rows // 2, model_width), lambda f: (0, 0))] * 2,
            scratch_shapes=[
                pltpu.VMEM((rows, model_width), jnp.bfloat16),
                pltpu.VMEM((hidden_width // h_tile, rows, h_tile), jnp.bfloat16),
                pltpu.VMEM((hidden_width, model_width), jnp.bfloat16),
                pltpu.SemaphoreType.DMA((n_tp + 1,)),
            ],
            compiler_params=pltpu.CompilerParams(
                dimension_semantics=("arbitrary",), vmem_limit_bytes=40 * 2**20
            ),
            cost_estimate=pl.CostEstimate(
                flops=6 * rows * model_width * hidden_width,
                transcendentals=rows * hidden_width,
                bytes_accessed=6 * model_width * hidden_width + 4 * rows * model_width,
            ),
            name="expert",
        )(*inputs, w_gate[0], w_up[0], w_down[0])
        added = swap(part_other, "tp", 1)

        def summed(j):
            here = slice(j * each, (j + 1) * each)
            return part_mine[here].astype(jnp.float32) + added[here].astype(jnp.float32)

        result = summed(0)
        for j in range(1, blocks):
            sent = swap(summed(j).astype(jnp.bfloat16), "tp", 2 * j)
            result = result + sent.astype(jnp.float32)
        returned.append(
            lax.all_to_all(result.astype(jnp.bfloat16), "sp", 0, 0, tiled=True)
        )

    def combine(*refs):
        combine_kernel(n_sp, *refs)

    return pl.pallas_call(
        combine,
        out_shape=jax.ShapeDtypeStruct((local_rows, model_width), jnp.bfloat16),
        in_specs=[vmem] * (3 + CHUNKS),
        out_specs=vmem,
        scratch_shapes=[pltpu.VMEM((n_sp * capacity, model_width), jnp.bfloat16)],
        compiler_params=pltpu.CompilerParams(vmem_limit_bytes=24 * 2**20),
        name="combine",
    )(stream, routes, route_weights, *returned)


def solution(mesh):
    in_specs = (
        P("sp", "tp"),
        P("sp", "tp"),
        P("sp", "tp"),
        P("sp", "tp"),
        P("sp"),
        P("tp"),
        P(),
        P(("sp", "tp"), None),
        P(),
        P(("sp", "tp"), None),
        P(("sp", "tp"), None),
        P("sp", None, "tp"),
        P("sp", None, "tp"),
        P("sp", "tp", None),
    )
    out_specs = P(("sp", "tp"), None)


    return jax.shard_map(on_device, mesh=mesh, in_specs=in_specs, out_specs=out_specs, check_vma=False)
```
